512 devices in a mesh: sp: 32 (over z, core), tp: 16 (over y, x).
Axes of the slice: x: 4, y: 4, z: 16, core: 2. Of those that a mesh axis runs over, the one named last changes fastest.
Arguments:
- tokens: bfloat16 [6144, 4096], P('sp', 'tp'), may hold values from -60 to 60
- lean_query: bfloat16 [6144, 16, 64], P('sp', 'tp'), may hold values from -6 to 6
- lean_key: bfloat16 [6144, 2, 64], P('sp'), may hold values from -6 to 6
- lean_value: bfloat16 [6144, 2, 64], P('sp'), may hold values from -6 to 6
- lean_gains: float32 [2, 64], replicated, may hold values from 0.25 to 7.5
- broad_query: bfloat16 [6144, 16, 128], P('sp', 'tp'), may hold values from -6 to 6
- broad_key: bfloat16 [6144, 2, 128], P('sp'), may hold values from -6 to 6
- broad_value: bfloat16 [6144, 2, 128], P('sp'), may hold values from -6 to 6
- broad_gains: float32 [2, 128], replicated, may hold values from 0.25 to 7.5
- mixer_gain: float32 [3072], replicated, may hold values from 0.1 to 1.9
- output_weight: bfloat16 [3072, 4096], P(None, 'tp'), may hold values from -0.109375 to 0.109375
- channel_gain: float32 [4096], P('tp'), may hold values from 0.1 to 1.9
- gate_weight: bfloat16 [32, 4096, 2048], P('sp', None, 'tp'), may hold values from -0.09375 to 0.09375
- up_weight: bfloat16 [32, 4096, 2048], P('sp', None, 'tp'), may hold values from -0.09375 to 0.09375
- down_weight: bfloat16 [32, 2048, 4096], P('sp', None, 'tp'), may hold values from -0.125 to 0.125
- route_experts: int32 [6144, 2], P('sp'), may hold values from 0 to 31, as said below
- route_logits: float32 [6144, 2], P('sp'), may hold values from -6 to 6
- group_weight: float32 [6144], P('sp'), may hold values from 0.3 to 1
Outputs:
- encoded: bfloat16 [6144, 4096], P('sp', 'tp')
The draws below stay inside these ranges and needn't reach their ends.
Inputs may be any that keep to these rules, and one draw needn't show every extreme that they name: `route_experts`: each row names two different experts of one group, expert e lying in group e // 8. In every aligned block of 192 rows no expert is named by more than 24 rows; one group, the same for all blocks, is named by exactly half of each block's rows, and each of its experts by exactly 24 of them.
All inputs are finite; a program needn't handle non-finite values.
Results may differ from the reference program's by a relative error of at most 0.0083.
Values may be sent and summed in bfloat16 or wider, within the bound.
A program may use at most 64 MiB of HBM per device.

```python
import jax
import jax.numpy as jnp
from jax import lax

TOK_SP = 192
SEQ = 6144
D = 4096
HQ_A = 16
KV_A = 2
HD_A = 64
HQ_B = 16
KV_B = 2
HD_B = 128
DMIX = 3072
GRID_W = 64
EXPERTS = 32
GROUPS = 4
EPG = 8
TOPK = 2
FF = 2048
CAP = 24
N_SP = 32


def drawn_pair(base_key, head_count, key_heads, head_size):
    subkeys = jax.random.split(base_key, 2)
    keys = jax.random.normal(subkeys[0], (SEQ, key_heads, head_size), jnp.float32)
    queries = jax.random.normal(subkeys[1], (SEQ, head_count, head_size), jnp.float32)
    return (jnp.clip(queries, -6.0, 6.0), jnp.clip(keys, -6.0, 6.0))


def gain_draw(base_key, head_size):
    return 1.0 + 0.18 * jnp.clip(jax.random.normal(base_key, (2, head_size), jnp.float32), -4.0, 4.0)


def draw_lean_query(key, part):
    return drawn_pair(jax.random.fold_in(key, 101), HQ_A, KV_A, HD_A)[0].astype(jnp.bfloat16)


def draw_lean_key(key, part):
    return drawn_pair(jax.random.fold_in(key, 101), HQ_A, KV_A, HD_A)[1].astype(jnp.bfloat16)


def draw_broad_query(key, part):
    return drawn_pair(jax.random.fold_in(key, 102), HQ_B, KV_B, HD_B)[0].astype(jnp.bfloat16)


def draw_broad_key(key, part):
    return drawn_pair(jax.random.fold_in(key, 102), HQ_B, KV_B, HD_B)[1].astype(jnp.bfloat16)


def draw_lean_gains(key, part):
    return gain_draw(jax.random.fold_in(key, 201), HD_A)


def draw_broad_gains(key, part):
    return gain_draw(jax.random.fold_in(key, 202), HD_B)


def draw_tokens(key, part):
    first_key, second_key = jax.random.split(jax.random.fold_in(key, 401))
    column = jnp.arange(D, dtype=jnp.float32) / D
    base_values = jnp.clip(jax.random.normal(first_key, (SEQ, D), jnp.float32), -5.0, 5.0)
    column_scale = 0.3 * 10.0 ** column
    row_scale = 0.4 * 10.0 ** jax.random.uniform(second_key, (SEQ, 1), jnp.float32)
    return (base_values * column_scale[None, :] * row_scale).astype(jnp.bfloat16)


def draw_route_experts(key, part):
    block_count = SEQ // TOK_SP
    half_rows = TOK_SP // 2
    big_group = jax.random.randint(jax.random.fold_in(key, 7), (), 0, GROUPS)
    block_keys = jax.random.split(jax.random.fold_in(key, 11), block_count)

    def one_block(block_key):
        cut_key, order_key, rank_key, inner_key = jax.random.split(block_key, 4)
        cut_points = jnp.sort(jax.random.randint(cut_key, (GROUPS - 2,), 0, half_rows + 1))
        bounds = jnp.concatenate([jnp.zeros((1,), jnp.int32), cut_points, jnp.full((1,), half_rows, jnp.int32)])
        starts = jnp.concatenate([jnp.zeros((1,), jnp.int32), half_rows + bounds[:-1]])
        ends = jnp.concatenate([jnp.full((1,), half_rows, jnp.int32), half_rows + bounds[1:]])
        others = (big_group + 1 + jax.random.permutation(order_key, GROUPS - 1)) % GROUPS
        group_order = jnp.concatenate([big_group[None], others])
        token_rank = jax.random.permutation(rank_key, TOK_SP)
        member = ((token_rank[:, None] >= starts[None, :]) & (token_rank[:, None] < ends[None, :])).astype(jnp.int32)
        which = jnp.argmax(member, axis=1)
        chosen_group = group_order[which]
        inner = token_rank - starts[which]
        first_pick = inner % EPG
        second_pick = (inner + 1 + inner // EPG % (EPG - 1)) % EPG
        shuffles = jax.vmap(lambda each_key: jax.random.permutation(each_key, EPG))(jax.random.split(inner_key, GROUPS))
        first_expert = chosen_group * EPG + shuffles[chosen_group, first_pick]
        second_expert = chosen_group * EPG + shuffles[chosen_group, second_pick]
        return jnp.stack([first_expert, second_expert], axis=1)
    return jax.vmap(one_block)(block_keys).reshape(SEQ, TOPK).astype(jnp.int32)


def shard_levels(rng, dims, pieces, low, high):
    loudness = 1.0
    for position, parts in pieces:
        draws = jax.random.uniform(jax.random.fold_in(jax.random.fold_in(rng, 6), position), (parts,), jnp.float32, low / len(pieces), high / len(pieces))
        loudness = loudness * jnp.repeat(jnp.exp(draws), dims[position] // parts).reshape((-1,) + (1,) * (len(dims) - 1 - position))
    return loudness


def gaussian(own_key, dims, spread, limit, cuts=(), kind=jnp.bfloat16):
    values = spread * jax.random.normal(own_key, dims, jnp.float32)
    if cuts:
        values = values * shard_levels(own_key, dims, cuts, -0.22, 0.18)
    return jnp.clip(values, -limit, limit).astype(kind)


def setup_inputs(seed: int = 0) -> dict:
    splits = jax.random.split(jax.random.key(seed), 19)
    return {
        "tokens": draw_tokens(jax.random.fold_in(splits[18], 71), 0),
        "lean_query": draw_lean_query(jax.random.fold_in(splits[18], 71), 0),
        "lean_key": draw_lean_key(jax.random.fold_in(splits[18], 71), 0),
        "lean_value": gaussian(splits[3], (SEQ, KV_A, HD_A), 1.0, 6.0, ((0, 32),)),
        "lean_gains": draw_lean_gains(jax.random.fold_in(splits[18], 71), 0),
        "broad_query": draw_broad_query(jax.random.fold_in(splits[18], 71), 0),
        "broad_key": draw_broad_key(jax.random.fold_in(splits[18], 71), 0),
        "broad_value": gaussian(splits[7], (SEQ, KV_B, HD_B), 1.0, 6.0, ((0, 32),)),
        "broad_gains": draw_broad_gains(jax.random.fold_in(splits[18], 71), 0),
        "mixer_gain": jnp.clip(1.0 + 0.18 * jax.random.normal(splits[9], (DMIX,), jnp.float32), 0.1, 1.9),
        "output_weight": gaussian(splits[10], (DMIX, D), DMIX ** -0.5, 0.109375, ((1, 16),)),
        "channel_gain": jnp.clip(1.0 + 0.18 * jax.random.normal(splits[11], (D,), jnp.float32), 0.1, 1.9),
        "gate_weight": gaussian(splits[12], (EXPERTS, D, FF), D ** -0.5, 0.09375, ((0, 32), (2, 16))),
        "up_weight": gaussian(splits[13], (EXPERTS, D, FF), D ** -0.5, 0.09375, ((0, 32), (2, 16))),
        "down_weight": gaussian(splits[14], (EXPERTS, FF, D), FF ** -0.5, 0.125, ((0, 32), (2, 16))),
        "route_experts": draw_route_experts(jax.random.fold_in(splits[18], 71), 0),
        "route_logits": gaussian(splits[16], (SEQ, TOPK), 1.5, 6.0, ((0, 32),), jnp.float32),
        "group_weight": jnp.clip(0.3 + 0.7 * jax.random.uniform(splits[17], (SEQ,), jnp.float32) ** shard_levels(splits[17], (SEQ,), ((0, 32),), -0.2, 0.2), 0.3, 1.0),
    }


epsilon = 1e-06
theta_base = 10000.0

def axial_angles(positions, head_size):
    quarter = head_size // 4
    frequency = theta_base ** (-jnp.arange(quarter, dtype=jnp.float32) / quarter)
    grid_rows = (positions // GRID_W).astype(jnp.float32)
    grid_columns = (positions % GRID_W).astype(jnp.float32)
    return (grid_rows[:, None] * frequency[None, :], grid_columns[:, None] * frequency[None, :])

def turn_half(values, angles):
    half_width = values.shape[-1] // 2
    first_half = values[..., :half_width]
    second = values[..., half_width:]
    cosine = jnp.cos(angles)[:, None, :]
    sine_part = jnp.sin(angles)[:, None, :]
    return jnp.concatenate([first_half * cosine - second * sine_part, second * cosine + first_half * sine_part], axis=-1)

def prepare(raw_values, gain_row, positions):
    values = raw_values.astype(jnp.float32)
    values = values * lax.rsqrt(lax.optimization_barrier(jnp.mean(values * values, axis=-1, keepdims=True)) + epsilon) * gain_row
    row_angles, column_angles = axial_angles(positions, raw_values.shape[-1])
    half_width = raw_values.shape[-1] // 2
    turned = jnp.concatenate([turn_half(values[..., :half_width], row_angles), turn_half(values[..., half_width:], column_angles)], axis=-1)
    return turned.astype(jnp.bfloat16)

def attend(queries, keys, values):
    token_count, head_count, head_size = queries.shape
    key_heads = keys.shape[1]
    group_ratio = head_count // key_heads
    blocks = queries.reshape(token_count // TOK_SP, TOK_SP, key_heads, group_ratio, head_size)
    keys_wide = keys.astype(jnp.float32)
    values_wide = values.astype(jnp.float32)

    def one_block(block_queries):
        scores = jnp.einsum('qkgd,skd->kgqs', block_queries.astype(jnp.float32), keys_wide) * head_size ** (-0.5)
        peak_score = lax.optimization_barrier(jnp.max(scores, axis=-1, keepdims=True))
        weights = jnp.exp(scores - peak_score)
        weight_sum = lax.optimization_barrier(jnp.sum(weights, axis=-1))
        rounded = lax.optimization_barrier(weights.astype(jnp.bfloat16)).astype(jnp.float32)
        summed = jnp.einsum('kgqs,skd->qkgd', rounded, values_wide)
        return (summed / jnp.transpose(weight_sum, (2, 0, 1))[..., None]).astype(jnp.bfloat16)
    mixed_heads = lax.map(one_block, blocks)
    return mixed_heads.reshape(token_count, head_count * head_size)

def group_norm(head_rows, gain_row):
    values = head_rows.astype(jnp.float32)
    return (values * lax.rsqrt(lax.optimization_barrier(jnp.mean(values * values, axis=-1, keepdims=True)) + epsilon) * gain_row).astype(jnp.bfloat16)

def reference(tokens, lean_query, lean_key, lean_value, lean_gains, broad_query, broad_key, broad_value, broad_gains, mixer_gain, output_weight, channel_gain, gate_weight, up_weight, down_weight, route_experts, route_logits, group_weight):
    positions = jnp.arange(SEQ, dtype=jnp.int32)
    lean_out = attend(prepare(lean_query, lean_gains[0], positions), prepare(lean_key, lean_gains[1], positions), lean_value)
    broad_out = attend(prepare(broad_query, broad_gains[0], positions), prepare(broad_key, broad_gains[1], positions), broad_value)
    lean_width = HQ_A * HD_A
    mixed_rows = jnp.concatenate([group_norm(lean_out, mixer_gain[:lean_width]), group_norm(broad_out, mixer_gain[lean_width:])], axis=1)
    stream = tokens.astype(jnp.float32) + jnp.dot(mixed_rows, output_weight, preferred_element_type=jnp.float32)
    normed = (stream * lax.rsqrt(lax.optimization_barrier(jnp.mean(stream * stream, axis=-1, keepdims=True)) + epsilon) * channel_gain).astype(jnp.bfloat16)
    logit_gap = route_logits[:, 0] - route_logits[:, 1]
    weights = group_weight[:, None] * jax.nn.sigmoid(jnp.stack([logit_gap, -logit_gap], axis=1))
    row_bound = N_SP * CAP

    def one_expert(running, expert_index):
        hit_mask = route_experts == expert_index
        member = jnp.any(hit_mask, axis=1)
        chosen = jnp.nonzero(member, size=row_bound, fill_value=0)[0]
        valid_rows = (jnp.arange(row_bound) < jnp.sum(member.astype(jnp.int32))).astype(jnp.float32)
        picked = normed[chosen]
        gate_value = jnp.dot(picked, gate_weight[expert_index], preferred_element_type=jnp.float32)
        up_value = jnp.dot(picked, up_weight[expert_index], preferred_element_type=jnp.float32)
        hidden = (jax.nn.silu(gate_value) * up_value).astype(jnp.bfloat16)
        result = jnp.dot(hidden, down_weight[expert_index], preferred_element_type=jnp.float32).astype(jnp.bfloat16)
        coefficient = lax.optimization_barrier(jnp.sum(jnp.where(hit_mask, weights, 0.0), axis=1))[chosen] * valid_rows
        return (running.at[chosen].add(coefficient[:, None] * result.astype(jnp.float32)), None)
    routed = lax.scan(one_expert, jnp.zeros((SEQ, D), jnp.float32), jnp.arange(EXPERTS, dtype=jnp.int32))[0]
    return (stream + routed).astype(jnp.bfloat16)
```

```python
import functools
import math

import jax
import jax.numpy as jnp
from jax import lax
from jax.experimental import pallas as pl
from jax.experimental.pallas import tpu as pltpu
from jax.sharding import Mesh
from jax.sharding import PartitionSpec as P

D = 4096
GRID_W = 64
KV = 2
GROUPS = 4
NY, NX = 4, 4
NCH = 4
HA, HB = 64, 128
FW = 256
FE = 128
MESH = pl.DeviceIdType.MESH
epsilon = 1e-06
theta_base = 10000.0
LOG2E = 1.4426950408889634


def axial_angles(positions, head_size):
    quarter = head_size // 4
    frequency = theta_base ** (-jnp.arange(quarter, dtype=jnp.float32) / quarter)
    grid_rows = (positions // GRID_W).astype(jnp.float32)
    grid_columns = (positions % GRID_W).astype(jnp.float32)
    return (grid_rows[:, None] * frequency[None, :], grid_columns[:, None] * frequency[None, :])


def turn_half(values, angles):
    half_width = values.shape[-1] // 2
    first_half = values[..., :half_width]
    second = values[..., half_width:]
    cosine = jnp.cos(angles)
    sine_part = jnp.sin(angles)
    return jnp.concatenate(
        [first_half * cosine - second * sine_part, second * cosine + first_half * sine_part],
        axis=-1,
    )


def prepare(raw_values, gain_row, positions):
    values = raw_values.astype(jnp.float32)
    values = (
        values * lax.rsqrt(jnp.mean(values * values, axis=-1, keepdims=True) + epsilon) * gain_row
    )
    row_angles, column_angles = axial_angles(positions, raw_values.shape[-1])
    half_width = raw_values.shape[-1] // 2
    turned = jnp.concatenate(
        [
            turn_half(values[..., :half_width], row_angles),
            turn_half(values[..., half_width:], column_angles),
        ],
        axis=-1,
    )
    return turned.astype(jnp.bfloat16)


def rcopy(src, dst, send_sem, recv_sem, device):
    return pltpu.make_async_remote_copy(
        src_ref=src,
        dst_ref=dst,
        send_sem=send_sem,
        recv_sem=recv_sem,
        device_id=device,
        device_id_type=MESH,
    )


def landed(ref, sem):
    pltpu.make_async_copy(ref, ref, sem).wait()


def dot_t(a, b):
    return lax.dot_general(a, b, (((1,), (1,)), ((), ())), preferred_element_type=jnp.float32)


def dot_n(a, b):
    return jnp.dot(a, b, preferred_element_type=jnp.float32)


def dot_exact(a, b, dims):
    return lax.dot_general(
        a,
        b,
        (dims, ((), ())),
        preferred_element_type=jnp.float32,
        precision=lax.Precision.HIGHEST,
    )


def layer_kernel(
    dims,
    q_ref,
    kv_ref,
    tok_ref,
    wl_ref,
    wb_ref,
    gate_ref,
    up_ref,
    down_ref,
    mg_ref,
    cg_ref,
    re_ref,
    rl_ref,
    gw_ref,
    o_ref,
    qbuf,
    kvbuf,
    osend,
    obuf,
    wo,
    wgu,
    wd,
    msend,
    mbuf,
    stsend,
    stbuf,
    psend,
    pbuf,
    st2send,
    st2buf,
    stream,
    sel0,
    sel1,
    outgo,
    xbuf,
    rsend,
    rbuf,
    gown,
    hbuf,
    dsend,
    dbuf,
    down_own,
    eout,
    ret,
    q_s,
    q_r,
    kv_s,
    kv_r,
    kv_f,
    o_s,
    o_r,
    wo_s,
    wo_r,
    wg_s,
    wg_r,
    wd_s,
    wd_r,
    loc,
    m_s,
    m_r,
    st_s,
    st_r,
    p_s,
    p_r,
    st2_s,
    st2_r,
    d_s,
    d_r,
    ya_s,
    ya_r,
    rx_s,
    rx_r,
    hx_s,
    hx_r,
    ry_s,
    ry_r,
    b_s,
    b_r,
):
    nz, ny, nx, t, cap = dims
    nsp = nz * 2
    ntp = ny * nx
    half = ny // KV
    grp = half * nx
    nb = nsp // grp
    cb = nsp // NCH
    rows = cb * cap
    z, c = lax.axis_index("z"), lax.axis_index("c")
    y, x = lax.axis_index("y"), lax.axis_index("x")
    s = z * 2 + c
    tp = y * nx + x
    head = y // half
    j = (y % half) * nx + x
    bf16, f32 = jnp.bfloat16, jnp.float32

    def member(g):
        return (z, c, head * half + g // nx, g % nx)

    def tp_dev(n):
        return (z, c, n // nx, n % nx)

    def sp_dev(n):
        return (n // 2, n % 2, y, x)

    barrier = pltpu.get_barrier_semaphore()
    for d in range(1, nsp):
        pl.semaphore_signal(barrier, inc=1, device_id=sp_dev((s + d) % nsp), device_id_type=MESH)
    for d in range(1, ntp):
        pl.semaphore_signal(barrier, inc=1, device_id=tp_dev((tp + d) % ntp), device_id_type=MESH)
    pl.semaphore_wait(barrier, nsp - 1 + ntp - 1)

    sends = []

    def send(src, dst, send_sem, recv_sem, device):
        copy = rcopy(src, dst, send_sem, recv_sem, device)
        copy.start()
        sends.append(copy)

    source = s % grp == j
    mine = s // grp
    order = [nz // 2]
    for d in range(nz // 2 - 1, 0, -1):
        order += [d, nz - d]

    @pl.when(source)
    def _():
        for n, d in enumerate(order):
            rcopy(
                kv_ref, kvbuf.at[mine], kv_s.at[n], kv_r.at[mine], ((z + d) % nz, mine % 2, y, x)
            ).start()
        rcopy(kv_ref, kvbuf.at[mine], kv_s.at[nz - 1], kv_r.at[mine], (z, 1 - c, y, x)).start()

    for d in range(1, grp):
        g = (j + d) % grp
        send(q_ref, qbuf.at[j], q_s.at[d], q_r.at[j], member(g))

    locals_ = []

    def local(src, dst, n):
        copy = pltpu.make_async_copy(src, dst, loc.at[n])
        copy.start()
        locals_.append(copy)

    local(wl_ref.at[pl.ds(y * nx, nx)], wo.at[y, :, 1], 0)
    local(wb_ref.at[pl.ds(ntp // 2 + y * nx, nx)], wo.at[y, :, pl.ds(2, 2)], 1)
    local(gate_ref.at[:, x], wgu.at[x, :, :, pl.ds(0, FE)], 2)
    local(up_ref.at[:, x], wgu.at[x, :, :, pl.ds(FE, FE)], 3)
    local(down_ref.at[y], wd.at[y], 4)
    for d in range(1, ny):
        to = (y + d) % ny
        dev = (z, c, to, x)
        send(
            wl_ref.at[pl.ds(to * nx, nx)], wo.at[y, :, 1], wo_s.at[0, d], wo_r.at[0, y], dev
        )
        send(
            wb_ref.at[pl.ds(ntp // 2 + to * nx, nx)],
            wo.at[y, :, pl.ds(2, 2)],
            wo_s.at[1, d],
            wo_r.at[1, y],
            dev,
        )
    for d in range(1, nx):
        to = (x + d) % nx
        dev = (z, c, y, to)
        send(gate_ref.at[:, to], wgu.at[x, :, :, pl.ds(0, FE)], wg_s.at[0, d], wg_r.at[0, x], dev)
        send(up_ref.at[:, to], wgu.at[x, :, :, pl.ds(FE, FE)], wg_s.at[1, d], wg_r.at[1, x], dev)
    for d in range(1, ny):
        to = (y + d) % ny
        send(down_ref.at[to], wd.at[y], wd_s.at[d], wd_r.at[y], (z, c, to, x))

    wo[:, :, 0] = jnp.zeros_like(wo[:, :, 0])
    qbuf[j] = q_ref[...]

    lane = lax.broadcasted_iota(jnp.int32, (t, 128), 1)
    e0 = (lane == re_ref[:, 0:1]).astype(f32)
    e1 = (lane == re_ref[:, 1:2]).astype(f32)
    before = (
        lax.broadcasted_iota(jnp.int32, (t, t), 0) > lax.broadcasted_iota(jnp.int32, (t, t), 1)
    ).astype(bf16)
    rank = dot_n(before, (e0 + e1).astype(bf16)) + (lane * cap).astype(f32)
    slot_lane = lax.broadcasted_iota(jnp.int32, (t, nsp * cap), 1)
    slot0 = jnp.sum(e0 * rank, axis=1, keepdims=True).astype(jnp.int32)
    slot1 = jnp.sum(e1 * rank, axis=1, keepdims=True).astype(jnp.int32)
    sel0[...] = (slot_lane == slot0).astype(f32).astype(bf16)
    sel1[...] = (slot_lane == slot1).astype(f32).astype(bf16)

    for i in range(nb):
        own = (mine == i) & source
        relay = (c == i % 2) & (z != (i * grp + j) // 2)

        @pl.when(own)
        def _():
            kvbuf[i] = kv_ref[...]

        @pl.when(jnp.logical_not(own))
        def _():
            landed(kvbuf.at[i], kv_r.at[i])

        @pl.when(relay)
        def _():
            rcopy(kvbuf.at[i], kvbuf.at[i], kv_f.at[i], kv_r.at[i], (z, 1 - c, y, x)).start()

    for d in range(1, grp):
        g = (j + d) % grp
        landed(qbuf.at[g], q_r.at[g])

    scale_a = HA**-0.5 * LOG2E
    scale_b = HB**-0.5 * LOG2E
    lane_a = lax.broadcasted_iota(jnp.int32, (t, 128), 1)

    def attend(scores, values, scale):
        peak = jnp.max(scores, axis=1, keepdims=True) * scale
        weights = jnp.exp2(scores * scale - peak)
        total = jnp.sum(weights, axis=1, keepdims=True)
        out = dot_n(weights.astype(bf16), values) / total
        return out, peak + jnp.log(total) * LOG2E

    def split3(v):
        a = v.astype(bf16).astype(f32)
        b = (v - a).astype(bf16).astype(f32)
        return a, b, v - a - b

    def one_head(d, carry):
        g = (j + d) % grp
        kv_l = kvbuf[:, :, 0:128].reshape(nb * t, 128)
        k_b = kvbuf[:, :, 128:256].reshape(nb * t, 128)
        v_b = kvbuf[:, :, 256:384].reshape(nb * t, 128)
        out_a, lse_a = attend(dot_t(qbuf[g, :, 0:128], kv_l), kv_l, scale_a)
        out_b, lse_b = attend(dot_t(qbuf[g, :, 128:256], k_b), v_b, scale_b)
        first = out_a
        for n, piece in enumerate(split3(lse_a) + split3(lse_b)):
            first = jnp.where(lane_a == n, piece, first)
        osend[g, :, 0:128] = first.astype(bf16)
        osend[g, :, 128:256] = out_b.astype(bf16)

        @pl.when(d < grp)
        def _():
            rcopy(osend.at[g], obuf.at[j], o_s.at[g], o_r.at[j], member(g)).start()

        @pl.when(d == grp)
        def _():
            obuf[j] = osend[g]

        return carry

    lax.fori_loop(1, grp + 1, one_head, 0)

    for d in range(1, grp):
        g = (j + d) % grp
        landed(obuf.at[g], o_r.at[g])

    lses = []
    for g in range(grp):
        stats = obuf[g, :, 0:128].astype(f32)
        lses.append(
            (
                stats[:, 0:1] + stats[:, 1:2] + stats[:, 2:3],
                stats[:, 3:4] + stats[:, 4:5] + stats[:, 5:6],
            )
        )
    top_a = functools.reduce(jnp.maximum, [v[0] for v in lses])
    top_b = functools.reduce(jnp.maximum, [v[1] for v in lses])
    sum_a, sum_b = 0.0, 0.0
    acc_a, acc_b = 0.0, 0.0
    for g in range(grp):
        wa = jnp.exp2(lses[g][0] - top_a)
        wb = jnp.exp2(lses[g][1] - top_b)
        sum_a, sum_b = sum_a + wa, sum_b + wb
        acc_a = acc_a + wa * obuf[g, :, 0:128].astype(f32)
        acc_b = acc_b + wb * obuf[g, :, 128:256].astype(f32)
    head_a = jnp.where(lane_a >= HA, acc_a / sum_a, 0.0).astype(bf16)
    head_b = (acc_b / sum_b).astype(bf16)
    msend[:, 0:128] = head_a
    msend[:, 128:256] = head_b
    for d in range(1, nx):
        to = (x + d) % nx
        send(msend, mbuf.at[x], m_s.at[d], m_r.at[x], (z, c, y, to))
    mbuf[x] = msend[...]
    row8 = lax.broadcasted_iota(jnp.int32, (8, 128), 0)
    pick_a = (row8 == 0).astype(f32)
    pick_b = (row8 == 1).astype(f32)
    sq_a, sq_b = head_a.astype(f32), head_b.astype(f32)
    last = ((1,), (1,))
    stsend[...] = jnp.zeros_like(stsend)
    stsend[:, 0:t] = dot_exact(pick_a, sq_a * sq_a, last) + dot_exact(pick_b, sq_b * sq_b, last)
    for d in range(1, ntp):
        n = (tp + d) % ntp
        send(stsend, stbuf.at[tp], st_s.at[d], st_r.at[tp], tp_dev(n))
    stbuf[tp] = stsend[...]
    for d in range(1, ntp):
        n = (tp + d) % ntp
        landed(stbuf.at[n], st_r.at[n])
    sums = jnp.sum(stbuf[...], axis=0)[:, 0:t]
    row_t = lax.broadcasted_iota(jnp.int32, (8, t), 0)
    width = jnp.where(row_t == 0, 1.0 / (ntp * HA), 1.0 / (ntp * HB))
    inverse = lax.rsqrt(sums * width + epsilon)
    first = ((0,), (0,))
    norm_a = dot_exact(inverse, pick_a, first)
    norm_b = dot_exact(inverse, pick_b, first)
    for d in range(1, nx):
        n = (x + d) % nx
        landed(mbuf.at[n], m_r.at[n])
    for copy in locals_:
        copy.wait()
    for d in range(1, ny):
        n = (y + d) % ny
        landed(wo.at[n, :, 1], wo_r.at[0, n])
        landed(wo.at[n, :, pl.ds(2, 2)], wo_r.at[1, n])
    for n in range(nx):
        gain = mg_ref[y * nx + n]
        part = mbuf[n]
        mbuf[n, :, 0:128] = (part[:, 0:128].astype(f32) * norm_a * gain[:, 0:128]).astype(bf16)
        mbuf[n, :, 128:256] = (part[:, 128:256].astype(f32) * norm_b * gain[:, 128:256]).astype(
            bf16
        )

    def project(n):
        acc = dot_n(mbuf[0], wo[n, 0].reshape(FW, FW))
        for m in range(1, nx):
            acc = acc + dot_n(mbuf[m], wo[n, m].reshape(FW, FW))
        return acc

    for d in range(1, ny):
        to = (y + d) % ny
        psend[d] = project(to).astype(bf16)
        send(psend.at[d], pbuf.at[y], p_s.at[d], p_r.at[y], (z, c, to, x))
    total = tok_ref[...].astype(f32) + project(y)
    for d in range(1, ny):
        n = (y + d) % ny
        landed(pbuf.at[n], p_r.at[n])
        total = total + pbuf[n].astype(f32)
    stream[...] = total
    ones8 = jnp.ones((8, FW), f32)
    st2send[...] = jnp.zeros_like(st2send)
    st2send[:, 0:t] = dot_exact(ones8, total * total, last)
    for d in range(1, ntp):
        n = (tp + d) % ntp
        send(st2send, st2buf.at[tp], st2_s.at[d], st2_r.at[tp], tp_dev(n))
    st2buf[tp] = st2send[...]
    for d in range(1, ntp):
        n = (tp + d) % ntp
        landed(st2buf.at[n], st2_r.at[n])
    squares = jnp.sum(st2buf[...], axis=0)[:, 0:t]
    inverse = lax.rsqrt(squares * (1.0 / (ntp * FW)) + epsilon)
    norm = dot_exact(inverse, jnp.where(row8 == 0, 1.0, 0.0), first)
    normed = (
        stream[...] * jnp.concatenate([norm, norm], axis=1) * cg_ref[...]
    ).astype(bf16)

    picked = lax.dot_general(
        sel0[...] + sel1[...], normed, (first, ((), ())), preferred_element_type=f32
    ).astype(bf16)
    for n in range(nsp):
        outgo[n] = picked[n * cap : (n + 1) * cap]
    for d in range(1, nsp):
        n = (s + d) % nsp
        send(outgo.at[n], xbuf.at[y, s], d_s.at[d], d_r.at[s], sp_dev(n))
    xbuf[y, s] = outgo[s]

    for d in range(1, nx):
        n = (x + d) % nx
        landed(wgu.at[n, :, :, pl.ds(0, FE)], wg_r.at[0, n])
        landed(wgu.at[n, :, :, pl.ds(FE, FE)], wg_r.at[1, n])
    for d in range(1, ny):
        n = (y + d) % ny
        landed(wd.at[n], wd_r.at[n])

    near = s // cb

    def chunk(k):
        return (near + k + k // 2 - 2 * (k // 3)) % NCH

    def stage_a(k):
        ch = chunk(k)
        for i in range(cb):
            b = ch * cb + i

            @pl.when(b != s)
            def _():
                landed(xbuf.at[y, b], d_r.at[b])

        part = xbuf.at[y, pl.ds(ch * cb, cb)]
        for d in range(1, ny):
            to = (y + d) % ny
            rcopy(part, part, ya_s.at[ch, d], ya_r.at[ch, y], (z, c, to, x)).start()

    def stage_b(k):
        ch = chunk(k)
        for d in range(1, ny):
            n = (y + d) % ny
            landed(xbuf.at[n, pl.ds(ch * cb, cb)], ya_r.at[ch, n])
        xs = [xbuf[n, pl.ds(ch * cb, cb)].reshape(rows, FW) for n in range(ny)]

        def expand(n):
            acc = dot_n(xs[0], wgu[n, 0])
            for m in range(1, ny):
                acc = acc + dot_n(xs[m], wgu[n, m])
            return acc

        for d in range(1, nx):
            to = (x + d) % nx
            rsend[ch, d] = expand(to).astype(bf16)
            rcopy(
                rsend.at[ch, d], rbuf.at[ch, x], rx_s.at[ch, d], rx_r.at[ch, x], (z, c, y, to)
            ).start()
        gown[ch] = expand(x)

    def stage_c(k):
        ch = chunk(k)
        both = gown[ch]
        for d in range(1, nx):
            n = (x + d) % nx
            landed(rbuf.at[ch, n], rx_r.at[ch, n])
            both = both + rbuf[ch, n].astype(f32)
        gate_value = both[:, 0:FE]
        hidden = (gate_value / (1.0 + jnp.exp(-gate_value)) * both[:, FE:]).astype(bf16)
        hbuf[ch, x] = hidden
        for d in range(1, nx):
            to = (x + d) % nx
            rcopy(
                hbuf.at[ch, x], hbuf.at[ch, x], hx_s.at[ch, d], hx_r.at[ch, x], (z, c, y, to)
            ).start()

    def stage_d(k):
        ch = chunk(k)
        for d in range(1, nx):
            n = (x + d) % nx
            landed(hbuf.at[ch, n], hx_r.at[ch, n])
        wide = jnp.concatenate([hbuf[ch, n] for n in range(nx)], axis=1)
        for d in range(1, ny):
            to = (y + d) % ny
            dsend[ch, d] = dot_n(wide, wd[to]).astype(bf16)
            rcopy(
                dsend.at[ch, d], dbuf.at[ch, y], ry_s.at[ch, d], ry_r.at[ch, y], (z, c, to, x)
            ).start()
        down_own[ch] = dot_n(wide, wd[y])

    def stage_e(k):
        ch = chunk(k)
        acc = down_own[ch]
        for d in range(1, ny):
            n = (y + d) % ny
            landed(dbuf.at[ch, n], ry_r.at[ch, n])
            acc = acc + dbuf[ch, n].astype(f32)
        eout[pl.ds(ch * cb, cb)] = acc.astype(bf16).reshape(cb, cap, FW)
        for i in range(cb):
            b = ch * cb + i

            @pl.when(b != s)
            def _():
                rcopy(eout.at[b], ret.at[s], b_s.at[b], b_r.at[s], sp_dev(b)).start()

            @pl.when(b == s)
            def _():
                ret[s] = eout[b]

    stages = (stage_a, stage_b, stage_c, stage_d, stage_e)

    def step(i, carry):
        for lag, stage in enumerate(stages):

            @pl.when((i >= lag) & (i < NCH + lag))
            def _():
                stage(i - lag)

        return carry

    lax.fori_loop(0, NCH + len(stages) - 1, step, 0)

    for d in range(1, nsp):
        n = (s + d) % nsp
        landed(ret.at[n], b_r.at[n])
    back = ret[...].reshape(nsp * cap, FW)
    gap = rl_ref[:, 0:1] - rl_ref[:, 1:2]
    w0 = gw_ref[...] / (1.0 + jnp.exp(-gap))
    w1 = gw_ref[...] / (1.0 + jnp.exp(gap))
    routed = w0 * dot_n(sel0[...], back) + w1 * dot_n(sel1[...], back)
    o_ref[...] = (stream[...] + routed).astype(bf16)

    for copy in sends:
        copy.wait_send()

    @pl.when(source)
    def _():
        for n in range(nz):
            landed(kv_ref, kv_s.at[n])

    for i in range(nb):
        relay = (c == i % 2) & (z != (i * grp + j) // 2)

        @pl.when(relay)
        def _():
            landed(kvbuf.at[i], kv_f.at[i])

    for d in range(1, grp):
        g = (j + d) % grp
        landed(osend.at[g], o_s.at[g])
    for ch in range(NCH):
        for d in range(1, ny):
            landed(xbuf.at[y, pl.ds(ch * cb, cb)], ya_s.at[ch, d])
            landed(dsend.at[ch, d], ry_s.at[ch, d])
        for d in range(1, nx):
            landed(rsend.at[ch, d], rx_s.at[ch, d])
            landed(hbuf.at[ch, x], hx_s.at[ch, d])
    for d in range(1, nsp):
        b = (s + d) % nsp
        landed(eout.at[b], b_s.at[b])


def on_device(
    tokens,
    lean_query,
    lean_key,
    lean_value,
    lean_gains,
    broad_query,
    broad_key,
    broad_value,
    broad_gains,
    mixer_gain,
    output_weight,
    channel_gain,
    gate_weight,
    up_weight,
    down_weight,
    route_experts,
    route_logits,
    group_weight,
):
    nz, ny, nx = lax.axis_size("z"), lax.axis_size("y"), lax.axis_size("x")
    nsp, ntp = nz * 2, ny * nx
    t = tokens.shape[0]
    cap = t // (nsp // GROUPS)
    half = ny // KV
    grp = half * nx
    nb = nsp // grp
    cb = nsp // NCH
    rows = cb * cap
    bf16, f32 = jnp.bfloat16, jnp.float32
    s = lax.axis_index("z") * 2 + lax.axis_index("c")
    head = lax.axis_index("y") // half
    positions = s * t + jnp.arange(t, dtype=jnp.int32)

    def own(array):
        return lax.dynamic_index_in_dim(array, head, 1, keepdims=False)

    q_all = jnp.concatenate(
        [
            prepare(lean_query[:, 0], lean_gains[0], positions),
            jnp.zeros((t, HA), bf16),
            prepare(broad_query[:, 0], broad_gains[0], positions),
        ],
        axis=1,
    )
    kv_all = jnp.concatenate(
        [
            prepare(own(lean_key), lean_gains[1], positions),
            own(lean_value),
            prepare(own(broad_key), broad_gains[1], positions),
            own(broad_value),
        ],
        axis=1,
    )
    gains = jnp.concatenate(
        [
            jnp.zeros((ntp, HA), f32),
            mixer_gain[: ntp * HA].reshape(ntp, HA),
            mixer_gain[ntp * HA :].reshape(ntp, HB),
        ],
        axis=1,
    ).reshape(ntp, 1, FW)
    vm = pl.BlockSpec(memory_space=pltpu.VMEM)
    hbm = pl.BlockSpec(memory_space=pl.ANY)
    dma = pltpu.SemaphoreType.DMA
    return pl.pallas_call(
        functools.partial(layer_kernel, (nz, ny, nx, t, cap)),
        out_shape=jax.ShapeDtypeStruct((t, FW), bf16),
        in_specs=[vm, vm, vm, hbm, hbm, hbm, hbm, hbm, vm, vm, vm, vm, vm],
        out_specs=vm,
        scratch_shapes=[
            pltpu.VMEM((grp, t, 256), bf16),
            pltpu.VMEM((nb, t, 384), bf16),
            pltpu.VMEM((grp, t, 256), bf16),
            pltpu.VMEM((grp, t, 256), bf16),
            pltpu.VMEM((ny, nx, 4, 64, FW), bf16),
            pltpu.VMEM((nx, ny, FW, FW), bf16),
            pltpu.VMEM((ny, nx * FE, FW), bf16),
            pltpu.VMEM((t, 256), bf16),
            pltpu.VMEM((nx, t, 256), bf16),
            pltpu.VMEM((8, 256), f32),
            pltpu.VMEM((ntp, 8, 256), f32),
            pltpu.VMEM((ny, t, FW), bf16),
            pltpu.VMEM((ny, t, FW), bf16),
            pltpu.VMEM((8, 256), f32),
            pltpu.VMEM((ntp, 8, 256), f32),
            pltpu.VMEM((t, FW), f32),
            pltpu.VMEM((t, nsp * cap), bf16),
            pltpu.VMEM((t, nsp * cap), bf16),
            pltpu.VMEM((nsp, cap, FW), bf16),
            pltpu.VMEM((ny, nsp, cap, FW), bf16),
            pltpu.VMEM((NCH, nx, rows, FW), bf16),
            pltpu.VMEM((NCH, nx, rows, FW), bf16),
            pltpu.VMEM((NCH, rows, FW), f32),
            pltpu.VMEM((NCH, nx, rows, FE), bf16),
            pltpu.VMEM((NCH, ny, rows, FW), bf16),
            pltpu.VMEM((NCH, ny, rows, FW), bf16),
            pltpu.VMEM((NCH, rows, FW), f32),
            pltpu.VMEM((nsp, cap, FW), bf16),
            pltpu.VMEM((nsp, cap, FW), bf16),
            dma((grp,)),
            dma((grp,)),
            dma((nz,)),
            dma((nb,)),
            dma((nb,)),
            dma((grp,)),
            dma((grp,)),
            dma((2, ny)),
            dma((2, ny)),
            dma((2, nx)),
            dma((2, nx)),
            dma((ny,)),
            dma((ny,)),
            dma((5,)),
            dma((nx,)),
            dma((nx,)),
            dma((ntp,)),
            dma((ntp,)),
            dma((ny,)),
            dma((ny,)),
            dma((ntp,)),
            dma((ntp,)),
            dma((nsp,)),
            dma((nsp,)),
            dma((NCH, ny)),
            dma((NCH, ny)),
            dma((NCH, nx)),
            dma((NCH, nx)),
            dma((NCH, nx)),
            dma((NCH, nx)),
            dma((NCH, ny)),
            dma((NCH, ny)),
            dma((nsp,)),
            dma((nsp,)),
        ],
        compiler_params=pltpu.CompilerParams(
            collective_id=0, has_side_effects=True, vmem_limit_bytes=60 * 1024 * 1024
        ),
    )(
        q_all,
        kv_all,
        tokens,
        output_weight.reshape(3 * ntp, 64, FW),
        output_weight.reshape(3 * ntp // 2, 2, 64, FW),
        gate_weight.reshape(ny, nx, FW, FE),
        up_weight.reshape(ny, nx, FW, FE),
        down_weight.reshape(ny, nx * FE, FW),
        gains,
        channel_gain.reshape(1, FW),
        route_experts,
        route_logits,
        group_weight.reshape(t, 1),
    )


def solution(mesh):
    finer = Mesh(
        mesh.devices.reshape(mesh.shape["sp"] // 2, 2, NY, NX), ("z", "c", "y", "x")
    )
    sp, tp = ("z", "c"), ("y", "x")
    return jax.shard_map(
        on_device,
        mesh=finer,
        in_specs=(
            P(sp, tp),
            P(sp, tp, None),
            P(sp, None, None),
            P(sp, None, None),
            P(),
            P(sp, tp, None),
            P(sp, None, None),
            P(sp, None, None),
            P(),
            P(),
            P(None, tp),
            P(tp),
            P(sp, None, tp),
            P(sp, None, tp),
            P(sp, None, tp),
            P(sp, None),
            P(sp, None),
            P(sp),
        ),
        out_specs=P(sp, tp),
        check_vma=False,
    )
```

```python
import functools
import math

import jax
import jax.numpy as jnp
from jax import lax
from jax.experimental import pallas as pl
from jax.experimental.pallas import tpu as pltpu
from jax.sharding import Mesh
from jax.sharding import PartitionSpec as P

D = 4096
GRID_W = 64
GRID_BITS = 6
KV = 2
GROUPS = 4
NY, NX = 4, 4
NCH = 4
HA, HB = 64, 128
FW = 256
FE = 128
MESH = pl.DeviceIdType.MESH
epsilon = 1e-06
theta_base = 10000.0
LOG2E = 1.4426950408889634


def rcopy(src, dst, send_sem, recv_sem, device):
    return pltpu.make_async_remote_copy(
        src_ref=src,
        dst_ref=dst,
        send_sem=send_sem,
        recv_sem=recv_sem,
        device_id=device,
        device_id_type=MESH,
    )


def landed(ref, sem):
    pltpu.make_async_copy(ref, ref, sem).wait()


def dot_t(a, b):
    return lax.dot_general(a, b, (((1,), (1,)), ((), ())), preferred_element_type=jnp.float32)


def dot_n(a, b):
    return jnp.dot(a, b, preferred_element_type=jnp.float32)


def dot_exact(a, b, dims):
    return lax.dot_general(
        a,
        b,
        (dims, ((), ())),
        preferred_element_type=jnp.float32,
        precision=lax.Precision.HIGHEST,
    )


def layer_kernel(
    dims,
    lq_ref,
    lk_ref,
    lv_ref,
    lg_ref,
    bq_ref,
    bk_ref,
    bv_ref,
    bg_ref,
    tok_ref,
    wl_ref,
    wb_ref,
    gate_ref,
    up_ref,
    down_ref,
    mg_ref,
    cg_ref,
    re_ref,
    rl_ref,
    gw_ref,
    o_ref,
    q_ref,
    kvl_ref,
    kvb_ref,
    qbuf,
    kvl,
    kvb,
    osend,
    obuf,
    wo,
    wgu,
    wd,
    msend,
    mbuf,
    stsend,
    stbuf,
    psend,
    pbuf,
    st2send,
    st2buf,
    stream,
    sel0,
    sel1,
    outgo,
    xbuf,
    rsend,
    rbuf,
    gown,
    hbuf,
    dsend,
    dbuf,
    down_own,
    eout,
    ret,
    q_s,
    q_r,
    kv_s,
    kv_r,
    kv_f,
    o_s,
    o_r,
    wo_s,
    wo_r,
    wg_s,
    wg_r,
    wd_s,
    wd_r,
    loc,
    m_s,
    m_r,
    st_s,
    st_r,
    p_s,
    p_r,
    st2_s,
    st2_r,
    d_s,
    d_r,
    ya_s,
    ya_r,
    rx_s,
    rx_r,
    hx_s,
    hx_r,
    ry_s,
    ry_r,
    b_s,
    b_r,
):
    nz, ny, nx, t, cap = dims
    nsp = nz * 2
    ntp = ny * nx
    half = ny // KV
    grp = half * nx
    nb = nsp // grp
    cb = nsp // NCH
    rows = cb * cap
    z, c = lax.axis_index("z"), lax.axis_index("c")
    y, x = lax.axis_index("y"), lax.axis_index("x")
    s = z * 2 + c
    tp = y * nx + x
    head = y // half
    j = (y % half) * nx + x
    bf16, f32 = jnp.bfloat16, jnp.float32

    def member(g):
        return (z, c, head * half + g // nx, g % nx)

    def tp_dev(n):
        return (z, c, n // nx, n % nx)

    def sp_dev(n):
        return (n // 2, n % 2, y, x)

    barrier = pltpu.get_barrier_semaphore()
    for d in range(1, nsp):
        pl.semaphore_signal(barrier, inc=1, device_id=sp_dev((s + d) % nsp), device_id_type=MESH)
    for d in range(1, ntp):
        pl.semaphore_signal(barrier, inc=1, device_id=tp_dev((tp + d) % ntp), device_id_type=MESH)

    def turned(raw, swapped, gain, size):
        quarter = size // 4
        lane = lax.broadcasted_iota(jnp.int32, (t, 128), 1)
        at = lax.broadcasted_iota(jnp.int32, (t, 128), 0) + s * t
        spot = jnp.where(lane < size // 2, at >> GRID_BITS, at & (GRID_W - 1)).astype(f32)
        step = (lane & (quarter - 1)).astype(f32) * (-math.log(theta_base) / quarter)
        angle = spot * jnp.exp(step)
        cosine = jnp.cos(angle)
        sine = jnp.where((lane & quarter) == 0, -1.0, 1.0) * jnp.sin(angle)
        results = []
        for (a, b), (g, h) in zip(zip(raw, swapped), gain):
            scale = lax.rsqrt(jnp.sum(a * a, axis=1, keepdims=True) * (1.0 / size) + epsilon)
            results.append(scale * (a * (g * cosine) + b * (h * sine)))
        return results

    def unit(size, shift):
        row = lax.broadcasted_iota(jnp.int32, (size, 128), 0)
        lane = lax.broadcasted_iota(jnp.int32, (size, 128), 1)
        return row + shift == lane, row == (lane ^ (size // 4))

    def gain_pair(ref, swap):
        pairs = dot_exact(ref[...], swap, ((1,), (0,)))
        return pairs[0:1], pairs[1:2]

    first = ((0,), (0,))

    def flipped(array, matrix):
        return lax.dot_general(array, matrix, (first, ((), ())), preferred_element_type=f32)

    same, swap = unit(HA, 0)
    place, _ = unit(HA, HA)
    same_b, swap_b, place_b = same.astype(bf16), swap.astype(bf16), place.astype(bf16)
    lk = lk_ref[head]
    g_raw, g_swap = gain_pair(lg_ref, same.astype(f32)), gain_pair(lg_ref, swap.astype(f32))
    q_a, k_a = turned(
        (flipped(lq_ref[...], same_b), flipped(lk, same_b)),
        (flipped(lq_ref[...], swap_b), flipped(lk, swap_b)),
        tuple(zip(g_raw, g_swap)),
        HA,
    )
    q_ref[:, 0:128] = q_a.astype(bf16)
    kvl_ref[...] = (k_a + flipped(lv_ref[head], place_b)).astype(bf16)
    _, swap = unit(HB, 0)
    swap_b = swap.astype(bf16)
    pair_row = lax.broadcasted_iota(jnp.int32, (t, KV * t), 0) * KV + head
    pick = (pair_row == lax.broadcasted_iota(jnp.int32, (t, KV * t), 1)).astype(bf16)
    k_raw = dot_n(pick, bk_ref[...])
    g_raw = (bg_ref[0:1], bg_ref[1:2])
    q_b, k_b = turned(
        (bq_ref[...].astype(f32), k_raw),
        (dot_n(bq_ref[...], swap_b), dot_n(k_raw.astype(bf16), swap_b)),
        tuple(zip(g_raw, gain_pair(bg_ref, swap.astype(f32)))),
        HB,
    )
    q_ref[:, 128:256] = q_b.astype(bf16)
    kvb_ref[:, 0:128] = k_b.astype(bf16)
    kvb_ref[:, 128:256] = dot_n(pick, bv_ref[...]).astype(bf16)

    experts = lax.broadcasted_iota(jnp.int32, (nsp, t), 0)
    e0 = (experts == re_ref[0:1]).astype(f32)
    e1 = (experts == re_ref[1:2]).astype(f32)
    before = (
        lax.broadcasted_iota(jnp.int32, (t, t), 0) < lax.broadcasted_iota(jnp.int32, (t, t), 1)
    ).astype(bf16)
    rank = dot_n((e0 + e1).astype(bf16), before) + (experts * cap).astype(f32)
    slot_row = lax.broadcasted_iota(jnp.int32, (nsp * cap, t), 0)
    slot0 = jnp.sum(e0 * rank, axis=0, keepdims=True).astype(jnp.int32)
    slot1 = jnp.sum(e1 * rank, axis=0, keepdims=True).astype(jnp.int32)
    sel0[...] = (slot_row == slot0).astype(f32).astype(bf16)
    sel1[...] = (slot_row == slot1).astype(f32).astype(bf16)
    wo[:, :, 0] = jnp.zeros_like(wo[:, :, 0])
    qbuf[j] = q_ref[...]

    pl.semaphore_wait(barrier, nsp - 1 + ntp - 1)

    sends = []

    def send(src, dst, send_sem, recv_sem, device):
        copy = rcopy(src, dst, send_sem, recv_sem, device)
        copy.start()
        sends.append(copy)

    source = s % grp == j
    mine = s // grp
    order = [nz // 2]
    for d in range(nz // 2 - 1, 0, -1):
        order += [d, nz - d]
    kv_pairs = ((kvl_ref, kvl), (kvb_ref, kvb))

    @pl.when(source)
    def _():
        for part, (src, dst) in enumerate(kv_pairs):
            for n, d in enumerate(order):
                rcopy(
                    src,
                    dst.at[mine],
                    kv_s.at[part, n],
                    kv_r.at[part, mine],
                    ((z + d) % nz, mine % 2, y, x),
                ).start()
            rcopy(
                src, dst.at[mine], kv_s.at[part, nz - 1], kv_r.at[part, mine], (z, 1 - c, y, x)
            ).start()

    for d in range(1, grp):
        g = (j + d) % grp
        send(q_ref, qbuf.at[j], q_s.at[d], q_r.at[j], member(g))

    locals_ = []

    def local(src, dst, n):
        copy = pltpu.make_async_copy(src, dst, loc.at[n])
        copy.start()
        locals_.append(copy)

    local(wl_ref.at[pl.ds(y * nx, nx)], wo.at[y, :, 1], 0)
    local(wb_ref.at[pl.ds(ntp // 2 + y * nx, nx)], wo.at[y, :, pl.ds(2, 2)], 1)
    local(gate_ref.at[:, x], wgu.at[x, :, :, pl.ds(0, FE)], 2)
    for d in range(1, ny):
        to = (y + d) % ny
        dev = (z, c, to, x)
        send(wl_ref.at[pl.ds(to * nx, nx)], wo.at[y, :, 1], wo_s.at[0, d], wo_r.at[0, y], dev)
        send(
            wb_ref.at[pl.ds(ntp // 2 + to * nx, nx)],
            wo.at[y, :, pl.ds(2, 2)],
            wo_s.at[1, d],
            wo_r.at[1, y],
            dev,
        )
    for d in range(1, nx):
        to = (x + d) % nx
        dev = (z, c, y, to)
        send(gate_ref.at[:, to], wgu.at[x, :, :, pl.ds(0, FE)], wg_s.at[0, d], wg_r.at[0, x], dev)

    def later_weights():
        for d in range(1, nx):
            to = (x + d) % nx
            dev = (z, c, y, to)
            send(
                up_ref.at[:, to], wgu.at[x, :, :, pl.ds(FE, FE)], wg_s.at[1, d], wg_r.at[1, x], dev
            )
        for d in range(1, ny):
            to = (y + d) % ny
            send(down_ref.at[to], wd.at[y], wd_s.at[d], wd_r.at[y], (z, c, to, x))

    local(up_ref.at[:, x], wgu.at[x, :, :, pl.ds(FE, FE)], 3)
    local(down_ref.at[y], wd.at[y], 4)

    def arrive(part):
        src, dst = kv_pairs[part]
        for i in range(nb):
            own = (mine == i) & source
            relay = (c == i % 2) & (z != (i * grp + j) // 2)

            @pl.when(own)
            def _():
                dst[i] = src[...]

            @pl.when(jnp.logical_not(own))
            def _():
                landed(dst.at[i], kv_r.at[part, i])

            @pl.when(relay)
            def _():
                rcopy(
                    dst.at[i], dst.at[i], kv_f.at[part, i], kv_r.at[part, i], (z, 1 - c, y, x)
                ).start()

    arrive(0)
    for d in range(1, grp):
        g = (j + d) % grp
        landed(qbuf.at[g], q_r.at[g])

    scale_a = HA**-0.5 * LOG2E
    scale_b = HB**-0.5 * LOG2E
    lane_a = lax.broadcasted_iota(jnp.int32, (t, 128), 1)

    def attend(scores, values, scale):
        peak = jnp.max(scores, axis=1, keepdims=True) * scale
        weights = jnp.exp2(scores * scale - peak)
        total = jnp.sum(weights, axis=1, keepdims=True)
        out = dot_n(weights.astype(bf16), values) / total
        return out, peak + jnp.log(total) * LOG2E

    def split3(v):
        a = v.astype(bf16).astype(f32)
        b = (v - a).astype(bf16).astype(f32)
        return a, b, v - a - b

    def marked(value, lse, at):
        for n, piece in enumerate(split3(lse)):
            value = jnp.where(lane_a == at + n, piece, value)
        return value

    def lean_head(g, carry):
        kv_l = kvl[...].reshape(nb * t, 128)
        out, lse = attend(dot_t(qbuf[g, :, 0:128], kv_l), kv_l, scale_a)
        osend[g, :, 0:128] = marked(out, lse, 0).astype(bf16)
        return carry

    def broad_head(d, carry):
        g = (j + d) % grp
        k_b = kvb[:, :, 0:128].reshape(nb * t, 128)
        v_b = kvb[:, :, 128:256].reshape(nb * t, 128)
        out, lse = attend(dot_t(qbuf[g, :, 128:256], k_b), v_b, scale_b)
        osend[g, :, 0:128] = marked(osend[g, :, 0:128].astype(f32), lse, 3).astype(bf16)
        osend[g, :, 128:256] = out.astype(bf16)

        @pl.when(d < grp)
        def _():
            rcopy(osend.at[g], obuf.at[j], o_s.at[g], o_r.at[j], member(g)).start()

        @pl.when(d == grp)
        def _():
            obuf[j] = osend[g]

        return carry

    lax.fori_loop(0, grp, lean_head, 0)
    arrive(1)
    lax.fori_loop(1, grp + 1, broad_head, 0)

    for d in range(1, grp):
        g = (j + d) % grp
        landed(obuf.at[g], o_r.at[g])

    lses = []
    for g in range(grp):
        stats = obuf[g, :, 0:128].astype(f32)
        lses.append(
            (
                stats[:, 0:1] + stats[:, 1:2] + stats[:, 2:3],
                stats[:, 3:4] + stats[:, 4:5] + stats[:, 5:6],
            )
        )
    top_a = functools.reduce(jnp.maximum, [v[0] for v in lses])
    top_b = functools.reduce(jnp.maximum, [v[1] for v in lses])
    sum_a, sum_b = 0.0, 0.0
    acc_a, acc_b = 0.0, 0.0
    for g in range(grp):
        wa = jnp.exp2(lses[g][0] - top_a)
        wb = jnp.exp2(lses[g][1] - top_b)
        sum_a, sum_b = sum_a + wa, sum_b + wb
        acc_a = acc_a + wa * obuf[g, :, 0:128].astype(f32)
        acc_b = acc_b + wb * obuf[g, :, 128:256].astype(f32)
    head_a = jnp.where(lane_a >= HA, acc_a / sum_a, 0.0).astype(bf16)
    head_b = (acc_b / sum_b).astype(bf16)
    msend[:, 0:128] = head_a
    msend[:, 128:256] = head_b
    row8 = lax.broadcasted_iota(jnp.int32, (8, 128), 0)
    pick_a = (row8 == 0).astype(f32)
    pick_b = (row8 == 1).astype(f32)
    sq_a, sq_b = head_a.astype(f32), head_b.astype(f32)
    last = ((1,), (1,))
    stsend[...] = jnp.zeros_like(stsend)
    stsend[:, 0:t] = dot_exact(pick_a, sq_a * sq_a, last) + dot_exact(pick_b, sq_b * sq_b, last)
    for d in range(1, ntp):
        n = (tp + d) % ntp
        send(stsend, stbuf.at[tp], st_s.at[d], st_r.at[tp], tp_dev(n))
    stbuf[tp] = stsend[...]
    for d in range(1, nx):
        to = (x + d) % nx
        send(msend, mbuf.at[x], m_s.at[d], m_r.at[x], (z, c, y, to))
    mbuf[x] = msend[...]
    for d in range(1, ntp):
        n = (tp + d) % ntp
        landed(stbuf.at[n], st_r.at[n])
    sums = jnp.sum(stbuf[...], axis=0)[:, 0:t]
    row_t = lax.broadcasted_iota(jnp.int32, (8, t), 0)
    width = jnp.where(row_t == 0, 1.0 / (ntp * HA), 1.0 / (ntp * HB))
    inverse = lax.rsqrt(sums * width + epsilon)
    norm_a = dot_exact(inverse, pick_a, first)
    norm_b = dot_exact(inverse, pick_b, first)
    for d in range(1, nx):
        n = (x + d) % nx
        landed(mbuf.at[n], m_r.at[n])
    for copy in locals_:
        copy.wait()
    for d in range(1, ny):
        n = (y + d) % ny
        landed(wo.at[n, :, 1], wo_r.at[0, n])
        landed(wo.at[n, :, pl.ds(2, 2)], wo_r.at[1, n])
    for n in range(nx):
        gain = mg_ref[pl.ds((y * nx + n) // 2, 1)]
        if n % 2 == 0:
            gain = pltpu.roll(gain, HA, 1)
        part = mbuf[n]
        mbuf[n, :, 0:128] = (part[:, 0:128].astype(f32) * norm_a * gain).astype(bf16)
        gain = mg_ref[pl.ds(ntp // 2 + y * nx + n, 1)]
        mbuf[n, :, 128:256] = (part[:, 128:256].astype(f32) * norm_b * gain).astype(bf16)

    def project(n):
        acc = dot_n(mbuf[0], wo[n, 0].reshape(FW, FW))
        for m in range(1, nx):
            acc = acc + dot_n(mbuf[m], wo[n, m].reshape(FW, FW))
        return acc

    for d in range(1, ny):
        to = (y + d) % ny
        psend[d] = project(to).astype(bf16)
        send(psend.at[d], pbuf.at[y], p_s.at[d], p_r.at[y], (z, c, to, x))
    total = tok_ref[...].astype(f32) + project(y)
    for d in range(1, ny):
        n = (y + d) % ny
        landed(pbuf.at[n], p_r.at[n])
        total = total + pbuf[n].astype(f32)
    stream[...] = total
    ones8 = jnp.ones((8, FW), f32)
    st2send[...] = jnp.zeros_like(st2send)
    st2send[:, 0:t] = dot_exact(ones8, total * total, last)
    for d in range(1, ntp):
        n = (tp + d) % ntp
        send(st2send, st2buf.at[tp], st2_s.at[d], st2_r.at[tp], tp_dev(n))
    st2buf[tp] = st2send[...]
    for d in range(1, ntp):
        n = (tp + d) % ntp
        landed(st2buf.at[n], st2_r.at[n])
    squares = jnp.sum(st2buf[...], axis=0)[:, 0:t]
    inverse = lax.rsqrt(squares * (1.0 / (ntp * FW)) + epsilon)
    norm = dot_exact(inverse, jnp.where(row8 == 0, 1.0, 0.0), first)
    normed = (
        stream[...] * jnp.concatenate([norm, norm], axis=1) * cg_ref[...]
    ).astype(bf16)

    picked = dot_n(sel0[...] + sel1[...], normed).astype(bf16)
    for n in range(nsp):
        outgo[n] = picked[n * cap : (n + 1) * cap]
    near = s // cb

    def dispatch(n):
        send(outgo.at[n], xbuf.at[y, s], d_s.at[n], d_r.at[s], sp_dev(n))

    for d in range(1, cb):
        dispatch(near * cb + (s + d) % cb)
    for i in range(cb):
        for d in (NCH - 1, 1)[: NCH - 1]:
            dispatch((near + d) % NCH * cb + i)
    for d in range(2, NCH - 1):
        for i in range(cb):
            dispatch((near + d) % NCH * cb + i)
    xbuf[y, s] = outgo[s]
    later_weights()

    for d in range(1, nx):
        n = (x + d) % nx
        landed(wgu.at[n, :, :, pl.ds(0, FE)], wg_r.at[0, n])
        landed(wgu.at[n, :, :, pl.ds(FE, FE)], wg_r.at[1, n])
    for d in range(1, ny):
        n = (y + d) % ny
        landed(wd.at[n], wd_r.at[n])

    def chunk(k):
        return (near + k + k // 2 - 2 * (k // 3)) % NCH

    def stage_a(k):
        ch = chunk(k)
        for i in range(cb):
            b = ch * cb + i

            @pl.when(b != s)
            def _():
                landed(xbuf.at[y, b], d_r.at[b])

        part = xbuf.at[y, pl.ds(ch * cb, cb)]
        for d in range(1, ny):
            to = (y + d) % ny
            rcopy(part, part, ya_s.at[ch, d], ya_r.at[ch, y], (z, c, to, x)).start()

    def stage_b(k):
        ch = chunk(k)
        for d in range(1, ny):
            n = (y + d) % ny
            landed(xbuf.at[n, pl.ds(ch * cb, cb)], ya_r.at[ch, n])
        xs = [xbuf[n, pl.ds(ch * cb, cb)].reshape(rows, FW) for n in range(ny)]

        def expand(n):
            acc = dot_n(xs[0], wgu[n, 0])
            for m in range(1, ny):
                acc = acc + dot_n(xs[m], wgu[n, m])
            return acc

        for d in range(1, nx):
            to = (x + d) % nx
            rsend[ch, d] = expand(to).astype(bf16)
            rcopy(
                rsend.at[ch, d], rbuf.at[ch, x], rx_s.at[ch, d], rx_r.at[ch, x], (z, c, y, to)
            ).start()
        gown[ch] = expand(x)

    def stage_c(k):
        ch = chunk(k)
        both = gown[ch]
        for d in range(1, nx):
            n = (x + d) % nx
            landed(rbuf.at[ch, n], rx_r.at[ch, n])
            both = both + rbuf[ch, n].astype(f32)
        gate_value = both[:, 0:FE]
        hidden = (gate_value / (1.0 + jnp.exp(-gate_value)) * both[:, FE:]).astype(bf16)
        hbuf[ch, x] = hidden
        for d in range(1, nx):
            to = (x + d) % nx
            rcopy(
                hbuf.at[ch, x], hbuf.at[ch, x], hx_s.at[ch, d], hx_r.at[ch, x], (z, c, y, to)
            ).start()

    def stage_d(k):
        ch = chunk(k)
        for d in range(1, nx):
            n = (x + d) % nx
            landed(hbuf.at[ch, n], hx_r.at[ch, n])
        wide = jnp.concatenate([hbuf[ch, n] for n in range(nx)], axis=1)
        for d in range(1, ny):
            to = (y + d) % ny
            dsend[ch, d] = dot_n(wide, wd[to]).astype(bf16)
            rcopy(
                dsend.at[ch, d], dbuf.at[ch, y], ry_s.at[ch, d], ry_r.at[ch, y], (z, c, to, x)
            ).start()
        down_own[ch] = dot_n(wide, wd[y])

    def stage_e(k):
        ch = chunk(k)
        acc = down_own[ch]
        for d in range(1, ny):
            n = (y + d) % ny
            landed(dbuf.at[ch, n], ry_r.at[ch, n])
            acc = acc + dbuf[ch, n].astype(f32)
        eout[pl.ds(ch * cb, cb)] = acc.astype(bf16).reshape(cb, cap, FW)
        for i in range(cb):
            b = ch * cb + i

            @pl.when(b != s)
            def _():
                rcopy(eout.at[b], ret.at[s], b_s.at[b], b_r.at[s], sp_dev(b)).start()

            @pl.when(b == s)
            def _():
                ret[s] = eout[b]


    stages = (stage_a, stage_b, stage_c, stage_d, stage_e)

    def step(i, carry):
        for lag, stage in enumerate(stages):

            @pl.when((i >= lag) & (i < NCH + lag))
            def _():
                stage(i - lag)

        return carry

    lax.fori_loop(0, NCH + len(stages) - 1, step, 0)

    for d in range(1, nsp):
        n = (s + d) % nsp
        landed(ret.at[n], b_r.at[n])
    back = ret[...].reshape(nsp * cap, FW)
    gap = rl_ref[0:1] - rl_ref[1:2]
    w0 = gw_ref[...] / (1.0 + jnp.exp(-gap))
    w1 = gw_ref[...] / (1.0 + jnp.exp(gap))
    both = jnp.where(row_t == 0, w0, jnp.where(row_t == 1, w1, 0.0))
    w0, w1 = dot_exact(both, pick_a, first), dot_exact(both, pick_b, first)
    w0, w1 = jnp.concatenate([w0, w0], axis=1), jnp.concatenate([w1, w1], axis=1)
    routed = w0 * flipped(sel0[...], back) + w1 * flipped(sel1[...], back)
    o_ref[...] = (stream[...] + routed).astype(bf16)

    for copy in sends:
        copy.wait_send()

    for part, (src, dst) in enumerate(kv_pairs):

        @pl.when(source)
        def _():
            for n in range(nz):
                landed(src, kv_s.at[part, n])

        for i in range(nb):
            relay = (c == i % 2) & (z != (i * grp + j) // 2)

            @pl.when(relay)
            def _():
                landed(dst.at[i], kv_f.at[part, i])

    for d in range(1, grp):
        g = (j + d) % grp
        landed(osend.at[g], o_s.at[g])
    for ch in range(NCH):
        for d in range(1, ny):
            landed(xbuf.at[y, pl.ds(ch * cb, cb)], ya_s.at[ch, d])
            landed(dsend.at[ch, d], ry_s.at[ch, d])
        for d in range(1, nx):
            landed(rsend.at[ch, d], rx_s.at[ch, d])
            landed(hbuf.at[ch, x], hx_s.at[ch, d])
    for d in range(1, nsp):
        b = (s + d) % nsp
        landed(eout.at[b], b_s.at[b])


def on_device(
    tokens,
    lean_query,
    lean_key,
    lean_value,
    lean_gains,
    broad_query,
    broad_key,
    broad_value,
    broad_gains,
    mixer_gain,
    output_weight,
    channel_gain,
    gate_weight,
    up_weight,
    down_weight,
    route_experts,
    route_logits,
    group_weight,
):
    nz, ny, nx = lax.axis_size("z"), lax.axis_size("y"), lax.axis_size("x")
    nsp, ntp = nz * 2, ny * nx
    t = tokens.shape[0]
    cap = t // (nsp // GROUPS)
    half = ny // KV
    grp = half * nx
    nb = nsp // grp
    cb = nsp // NCH
    rows = cb * cap
    bf16, f32 = jnp.bfloat16, jnp.float32
    vm = pl.BlockSpec(memory_space=pltpu.VMEM)
    hbm = pl.BlockSpec(memory_space=pl.ANY)
    dma = pltpu.SemaphoreType.DMA
    return pl.pallas_call(
        functools.partial(layer_kernel, (nz, ny, nx, t, cap)),
        out_shape=jax.ShapeDtypeStruct((t, FW), bf16),
        in_specs=[vm] * 9 + [hbm] * 5 + [vm] * 5,
        out_specs=vm,
        scratch_shapes=[
            pltpu.VMEM((t, 256), bf16),
            pltpu.VMEM((t, 128), bf16),
            pltpu.VMEM((t, 256), bf16),
            pltpu.VMEM((grp, t, 256), bf16),
            pltpu.VMEM((nb, t, 128), bf16),
            pltpu.VMEM((nb, t, 256), bf16),
            pltpu.VMEM((grp, t, 256), bf16),
            pltpu.VMEM((grp, t, 256), bf16),
            pltpu.VMEM((ny, nx, 4, 64, FW), bf16),
            pltpu.VMEM((nx, ny, FW, FW), bf16),
            pltpu.VMEM((ny, nx * FE, FW), bf16),
            pltpu.VMEM((t, 256), bf16),
            pltpu.VMEM((nx, t, 256), bf16),
            pltpu.VMEM((8, 256), f32),
            pltpu.VMEM((ntp, 8, 256), f32),
            pltpu.VMEM((ny, t, FW), bf16),
            pltpu.VMEM((ny, t, FW), bf16),
            pltpu.VMEM((8, 256), f32),
            pltpu.VMEM((ntp, 8, 256), f32),
            pltpu.VMEM((t, FW), f32),
            pltpu.VMEM((nsp * cap, t), bf16),
            pltpu.VMEM((nsp * cap, t), bf16),
            pltpu.VMEM((nsp, cap, FW), bf16),
            pltpu.VMEM((ny, nsp, cap, FW), bf16),
            pltpu.VMEM((NCH, nx, rows, FW), bf16),
            pltpu.VMEM((NCH, nx, rows, FW), bf16),
            pltpu.VMEM((NCH, rows, FW), f32),
            pltpu.VMEM((NCH, nx, rows, FE), bf16),
            pltpu.VMEM((NCH, ny, rows, FW), bf16),
            pltpu.VMEM((NCH, ny, rows, FW), bf16),
            pltpu.VMEM((NCH, rows, FW), f32),
            pltpu.VMEM((nsp, cap, FW), bf16),
            pltpu.VMEM((nsp, cap, FW), bf16),
            dma((grp,)),
            dma((grp,)),
            dma((2, nz)),
            dma((2, nb)),
            dma((2, nb)),
            dma((grp,)),
            dma((grp,)),
            dma((2, ny)),
            dma((2, ny)),
            dma((2, nx)),
            dma((2, nx)),
            dma((ny,)),
            dma((ny,)),
            dma((5,)),
            dma((nx,)),
            dma((nx,)),
            dma((ntp,)),
            dma((ntp,)),
            dma((ny,)),
            dma((ny,)),
            dma((ntp,)),
            dma((ntp,)),
            dma((nsp,)),
            dma((nsp,)),
            dma((NCH, ny)),
            dma((NCH, ny)),
            dma((NCH, nx)),
            dma((NCH, nx)),
            dma((NCH, nx)),
            dma((NCH, nx)),
            dma((NCH, ny)),
            dma((NCH, ny)),
            dma((nsp,)),
            dma((nsp,)),
        ],
        compiler_params=pltpu.CompilerParams(
            collective_id=0, has_side_effects=True, vmem_limit_bytes=60 * 1024 * 1024
        ),
    )(
        lean_query.transpose(1, 2, 0)[0],
        lean_key.transpose(1, 2, 0),
        lean_value.transpose(1, 2, 0),
        lean_gains,
        broad_query[:, 0],
        broad_key.reshape(KV * t, HB),
        broad_value.reshape(KV * t, HB),
        broad_gains,
        tokens,
        output_weight.reshape(3 * ntp, 64, FW),
        output_weight.reshape(3 * ntp // 2, 2, 64, FW),
        gate_weight.reshape(ny, nx, FW, FE),
        up_weight.reshape(ny, nx, FW, FE),
        down_weight.reshape(ny, nx * FE, FW),
        mixer_gain.reshape(-1, 128),
        channel_gain.reshape(1, FW),
        route_experts.T,
        route_logits.T,
        group_weight.reshape(1, t),
    )


def solution(mesh):
    finer = Mesh(
        mesh.devices.reshape(mesh.shape["sp"] // 2, 2, NY, NX), ("z", "c", "y", "x")
    )
    sp, tp = ("z", "c"), ("y", "x")
    return jax.shard_map(
        on_device,
        mesh=finer,
        in_specs=(
            P(sp, tp),
            P(sp, tp, None),
            P(sp, None, None),
            P(sp, None, None),
            P(),
            P(sp, tp, None),
            P(sp, None, None),
            P(sp, None, None),
            P(),
            P(),
            P(None, tp),
            P(tp),
            P(sp, None, tp),
            P(sp, None, tp),
            P(sp, None, tp),
            P(sp, None),
            P(sp, None),
            P(sp),
        ),
        out_specs=P(sp, tp),
        check_vma=False,
    )
```

```python
import functools
import math

import jax
import jax.numpy as jnp
from jax import lax
from jax.experimental import pallas as pl
from jax.experimental.pallas import tpu as pltpu
from jax.sharding import Mesh
from jax.sharding import PartitionSpec as P

D = 4096
GRID_W = 64
GRID_BITS = 6
KV = 2
GROUPS = 4
NY, NX = 4, 4
NCH = 4
HUBS = (8, 5, 11, 2, 14)
UNROLL = 2
HA, HB = 64, 128
FW = 256
FE = 128
MESH = pl.DeviceIdType.MESH
epsilon = 1e-06
theta_base = 10000.0
LOG2E = 1.4426950408889634


def rcopy(src, dst, send_sem, recv_sem, device):
    return pltpu.make_async_remote_copy(
        src_ref=src,
        dst_ref=dst,
        send_sem=send_sem,
        recv_sem=recv_sem,
        device_id=device,
        device_id_type=MESH,
    )


def landed(ref, sem):
    pltpu.make_async_copy(ref, ref, sem).wait()


def dot_t(a, b):
    return lax.dot_general(a, b, (((1,), (1,)), ((), ())), preferred_element_type=jnp.float32)


def dot_n(a, b):
    return jnp.dot(a, b, preferred_element_type=jnp.float32)


def dot_exact(a, b, dims):
    return lax.dot_general(
        a,
        b,
        (dims, ((), ())),
        preferred_element_type=jnp.float32,
        precision=lax.Precision.HIGHEST,
    )


def layer_kernel(
    dims,
    lq_ref,
    lk_ref,
    lv_ref,
    lg_ref,
    bq_ref,
    bk_ref,
    bv_ref,
    bg_ref,
    tok_ref,
    wl_ref,
    wb_ref,
    gate_ref,
    up_ref,
    down_ref,
    mg_ref,
    cg_ref,
    re_ref,
    rl_ref,
    gw_ref,
    o_ref,
    q_ref,
    kvl_ref,
    kvb_ref,
    qbuf,
    kvl,
    kvb,
    osl,
    osb,
    obl,
    obb,
    lsend,
    lbuf,
    wo,
    wgu,
    wd,
    msend,
    mbuf,
    stsend,
    stbuf,
    psend,
    pbuf,
    st2send,
    st2buf,
    stream,
    sel0,
    sel1,
    sel_wide,
    scsend,
    scbuf,
    outgo,
    xbuf,
    rsend,
    rbuf,
    gown,
    hbuf,
    dsend,
    dbuf,
    down_own,
    eout,
    ret,
    q_s,
    q_r,
    kv_s,
    kv_r,
    kv_f,
    o_s,
    o_r,
    wo_s,
    wo_r,
    wg_s,
    wg_r,
    wd_s,
    wd_r,
    loc,
    m_s,
    m_r,
    st_s,
    st_r,
    p_s,
    p_r,
    st2_s,
    st2_r,
    d_s,
    d_r,
    sc_s,
    sc_r,
    ya_s,
    ya_r,
    rx_s,
    rx_r,
    hx_s,
    hx_r,
    ry_s,
    ry_r,
    b_s,
    b_r,
):
    nz, ny, nx, t, cap = dims
    nsp = nz * 2
    ntp = ny * nx
    half = ny // KV
    grp = nx
    nb = nsp // grp
    cb = nsp // NCH
    rows = cb * cap
    wide = 32 if cap <= 32 else 128
    per = 128 // wide
    z, c = lax.axis_index("z"), lax.axis_index("c")
    y, x = lax.axis_index("y"), lax.axis_index("x")
    s = z * 2 + c
    tp = y * nx + x
    head = y // half
    j = x
    bf16, f32 = jnp.bfloat16, jnp.float32

    def member(g):
        return (z, c, y, g)

    def tp_dev(n):
        return (z, c, n // nx, n % nx)

    def sp_dev(n):
        return (n // 2, n % 2, y, x)

    barrier = pltpu.get_barrier_semaphore()
    for d in range(1, nsp):
        pl.semaphore_signal(barrier, inc=1, device_id=sp_dev((s + d) % nsp), device_id_type=MESH)
    for d in range(1, ntp):
        pl.semaphore_signal(barrier, inc=1, device_id=tp_dev((tp + d) % ntp), device_id_type=MESH)

    def turned(raw, swapped, gain, size):
        quarter = size // 4
        lane = lax.broadcasted_iota(jnp.int32, (t, 128), 1)
        at = lax.broadcasted_iota(jnp.int32, (t, 128), 0) + s * t
        spot = jnp.where(lane < size // 2, at >> GRID_BITS, at & (GRID_W - 1)).astype(f32)
        step = (lane & (quarter - 1)).astype(f32) * (-math.log(theta_base) / quarter)
        angle = spot * jnp.exp(step)
        cosine = jnp.cos(angle)
        sine = jnp.where((lane & quarter) == 0, -1.0, 1.0) * jnp.sin(angle)
        results = []
        for (a, b), (g, h) in zip(zip(raw, swapped), gain):
            scale = lax.rsqrt(jnp.sum(a * a, axis=1, keepdims=True) * (1.0 / size) + epsilon)
            results.append(scale * (a * (g * cosine) + b * (h * sine)))
        return results

    def unit(size, shift):
        row = lax.broadcasted_iota(jnp.int32, (size, 128), 0)
        lane = lax.broadcasted_iota(jnp.int32, (size, 128), 1)
        return row + shift == lane, row == (lane ^ (size // 4))

    def gain_pair(ref, swap):
        pairs = dot_exact(ref[...], swap, ((1,), (0,)))
        return pairs[0:1], pairs[1:2]

    first = ((0,), (0,))

    def flipped(array, matrix):
        return lax.dot_general(array, matrix, (first, ((), ())), preferred_element_type=f32)

    same, swap = unit(HA, 0)
    place, _ = unit(HA, HA)
    same_b, swap_b, place_b = same.astype(bf16), swap.astype(bf16), place.astype(bf16)
    lk = lk_ref[head]
    g_raw, g_swap = gain_pair(lg_ref, same.astype(f32)), gain_pair(lg_ref, swap.astype(f32))
    q_a, k_a = turned(
        (flipped(lq_ref[...], same_b), flipped(lk, same_b)),
        (flipped(lq_ref[...], swap_b), flipped(lk, swap_b)),
        tuple(zip(g_raw, g_swap)),
        HA,
    )
    q_ref[:, 0:128] = q_a.astype(bf16)
    kvl_ref[...] = (k_a + flipped(lv_ref[head], place_b)).astype(bf16)
    _, swap = unit(HB, 0)
    swap_b = swap.astype(bf16)
    pair_row = lax.broadcasted_iota(jnp.int32, (t, KV * t), 0) * KV + head
    pick = (pair_row == lax.broadcasted_iota(jnp.int32, (t, KV * t), 1)).astype(bf16)
    k_raw = dot_n(pick, bk_ref[...])
    g_raw = (bg_ref[0:1], bg_ref[1:2])
    q_b, k_b = turned(
        (bq_ref[...].astype(f32), k_raw),
        (dot_n(bq_ref[...], swap_b), dot_n(k_raw.astype(bf16), swap_b)),
        tuple(zip(g_raw, gain_pair(bg_ref, swap.astype(f32)))),
        HB,
    )
    q_ref[:, 128:256] = q_b.astype(bf16)
    kvb_ref[:, 0:128] = k_b.astype(bf16)
    kvb_ref[:, 128:256] = dot_n(pick, bv_ref[...]).astype(bf16)

    experts = lax.broadcasted_iota(jnp.int32, (nsp, t), 0)
    e0 = (experts == re_ref[0:1]).astype(f32)
    e1 = (experts == re_ref[1:2]).astype(f32)
    before = (
        lax.broadcasted_iota(jnp.int32, (t, t), 0) < lax.broadcasted_iota(jnp.int32, (t, t), 1)
    ).astype(bf16)
    rank = dot_n((e0 + e1).astype(bf16), before)

    def slots(pitch):
        row = lax.broadcasted_iota(jnp.int32, (nsp * pitch, t), 0)
        place = rank + (experts * pitch).astype(f32)
        for e in (e0, e1):
            slot = jnp.sum(e * place, axis=0, keepdims=True).astype(jnp.int32)
            yield (row == slot).astype(f32)

    for part, sel in zip(slots(cap), (sel0, sel1)):
        sel[...] = part.astype(bf16)
    sel_wide[...] = sum(slots(wide)).astype(bf16)
    wo[:, :, 0] = jnp.zeros_like(wo[:, :, 0])
    qbuf[j] = q_ref[...]

    pl.semaphore_wait(barrier, nsp - 1 + ntp - 1)

    sends = []

    def send(src, dst, send_sem, recv_sem, device):
        copy = rcopy(src, dst, send_sem, recv_sem, device)
        copy.start()
        sends.append(copy)

    source = s % grp == j
    mine = s // grp
    hubs = HUBS if nz == 16 else tuple(range(1, nz))
    kv_pairs = ((kvl_ref, kvl), (kvb_ref, kvb))

    @pl.when(source)
    def _():
        for part, (src, dst) in enumerate(kv_pairs):
            for n, d in enumerate(hubs):
                rcopy(
                    src,
                    dst.at[mine],
                    kv_s.at[part, n],
                    kv_r.at[part, mine],
                    ((z + d) % nz, mine % 2, y, x),
                ).start()
            rcopy(
                src, dst.at[mine], kv_s.at[part, nz - 1], kv_r.at[part, mine], (z, 1 - c, y, x)
            ).start()

    for d in range(1, grp):
        g = (j + d) % grp
        send(q_ref, qbuf.at[j], q_s.at[d], q_r.at[j], member(g))

    locals_ = []

    def local(src, dst, n):
        copy = pltpu.make_async_copy(src, dst, loc.at[n])
        copy.start()
        locals_.append(copy)

    local(wl_ref.at[pl.ds(y * nx, nx)], wo.at[y, :, 1], 0)
    local(wb_ref.at[pl.ds(ntp // 2 + y * nx, nx)], wo.at[y, :, pl.ds(2, 2)], 1)
    local(gate_ref.at[:, x], wgu.at[x, :, :, pl.ds(0, FE)], 2)
    for d in range(1, ny):
        to = (y + d) % ny
        dev = (z, c, to, x)
        send(wl_ref.at[pl.ds(to * nx, nx)], wo.at[y, :, 1], wo_s.at[0, d], wo_r.at[0, y], dev)
        send(
            wb_ref.at[pl.ds(ntp // 2 + to * nx, nx)],
            wo.at[y, :, pl.ds(2, 2)],
            wo_s.at[1, d],
            wo_r.at[1, y],
            dev,
        )
    for d in range(1, nx):
        to = (x + d) % nx
        dev = (z, c, y, to)
        send(gate_ref.at[:, to], wgu.at[x, :, :, pl.ds(0, FE)], wg_s.at[0, d], wg_r.at[0, x], dev)

    def send_up(d):
        to = (x + d) % nx
        dev = (z, c, y, to)
        send(up_ref.at[:, to], wgu.at[x, :, :, pl.ds(FE, FE)], wg_s.at[1, d], wg_r.at[1, x], dev)

    near_x = sorted({1, nx - 1})
    for d in near_x:
        send_up(d)

    for d in range(1, ny):
        to = (y + d) % ny
        send(down_ref.at[to], wd.at[y], wd_s.at[d], wd_r.at[y], (z, c, to, x))

    local(up_ref.at[:, x], wgu.at[x, :, :, pl.ds(FE, FE)], 3)
    local(down_ref.at[y], wd.at[y], 4)

    def away(i):
        return (z - (i * grp + j) // 2 + nz) % nz

    def hub(i):
        return (c == i % 2) & (away(i) % 3 == 2) if nz == 16 else away(i) < 0

    def pass_on(part, i):
        dst = kv_pairs[part][1]
        landed(dst.at[i], kv_r.at[part, i])

        @pl.when((c == i % 2) & (away(i) != 0))
        def _():
            rcopy(
                dst.at[i], dst.at[i], kv_f.at[part, i, 0], kv_r.at[part, i], (z, 1 - c, y, x)
            ).start()

    def arrive_first(part):
        src, dst = kv_pairs[part]
        for i in range(nb):

            @pl.when((mine == i) & source)
            def _():
                dst[i] = src[...]

            @pl.when(hub(i))
            def _():
                pass_on(part, i)
                for n, d in ((1, 1), (2, nz - 1)):
                    rcopy(
                        dst.at[i],
                        dst.at[i],
                        kv_f.at[part, i, n],
                        kv_r.at[part, i],
                        ((z + d) % nz, c, y, x),
                    ).start()

    def arrive(part):
        for i in range(nb):
            direct = ((mine == i) & source) | hub(i)

            @pl.when(jnp.logical_not(direct))
            def _():
                pass_on(part, i)

    arrive_first(0)
    arrive(0)
    arrive_first(1)
    for d in range(1, grp):
        g = (j + d) % grp
        landed(qbuf.at[g], q_r.at[g])

    scale_a = HA**-0.5 * LOG2E
    scale_b = HB**-0.5 * LOG2E
    lane_a = lax.broadcasted_iota(jnp.int32, (t, 128), 1)

    def attend(scores, values, scale):
        peak = jnp.max(scores, axis=1, keepdims=True) * scale
        weights = jnp.exp2(scores * scale - peak)
        total = jnp.sum(weights, axis=1, keepdims=True)
        out = dot_n(weights.astype(bf16), values) / total
        return out, peak + jnp.log(total) * LOG2E

    def split3(v):
        a = v.astype(bf16).astype(f32)
        b = (v - a).astype(bf16).astype(f32)
        return a, b, v - a - b

    def marked(value, lse, at):
        for n, piece in enumerate(split3(lse)):
            value = jnp.where(lane_a == at + n, piece, value)
        return value

    def hand_over(part, src, dst, d, g):
        @pl.when(d < grp)
        def _():
            rcopy(src.at[g], dst.at[j], o_s.at[part, g], o_r.at[part, j], member(g)).start()

        @pl.when(d == grp)
        def _():
            dst[j] = src[g]

    def lean_head(d, carry):
        g = (j + d) % grp
        kv_l = kvl[...].reshape(nb * t, 128)
        out, lse = attend(dot_t(qbuf[g, :, 0:128], kv_l), kv_l, scale_a)
        osl[g] = marked(out, lse, 0).astype(bf16)
        hand_over(0, osl, obl, d, g)
        return carry

    def broad_head(d, lses):
        g = (j + d) % grp
        k_b = kvb[:, :, 0:128].reshape(nb * t, 128)
        v_b = kvb[:, :, 128:256].reshape(nb * t, 128)
        out, lse = attend(dot_t(qbuf[g, :, 128:256], k_b), v_b, scale_b)
        osb[g] = out.astype(bf16)
        hand_over(1, osb, obb, d, g)
        return jnp.where(lane_a == g, lse, lses)

    lax.fori_loop(1, grp + 1, lean_head, 0, unroll=UNROLL)
    arrive(1)
    lses = lax.fori_loop(1, grp + 1, broad_head, jnp.zeros((t, 128), f32), unroll=UNROLL)
    last = ((1,), (1,))
    row8 = lax.broadcasted_iota(jnp.int32, (8, 128), 0)
    eye8 = (row8 == lax.broadcasted_iota(jnp.int32, (8, 128), 1)).astype(f32)
    lsend[...] = jnp.zeros_like(lsend)
    lse_rows = dot_exact(eye8, lses, last)
    for g in range(grp):
        lsend[g, :, 0:t] = lse_rows[g : g + 1]
    for d in range(1, grp):
        g = (j + d) % grp
        send(lsend.at[g], lbuf.at[j], o_s.at[2, g], o_r.at[2, j], member(g))
    lbuf[j] = lsend[j]

    for d in range(1, grp):
        g = (j + d) % grp
        landed(obl.at[g], o_r.at[0, g])
        landed(obb.at[g], o_r.at[1, g])
        landed(lbuf.at[g], o_r.at[2, g])

    row_g = lax.broadcasted_iota(jnp.int32, (8, t), 0)
    lse_rows = jnp.zeros((8, t), f32)
    for g in range(grp):
        lse_rows = jnp.where(row_g == g, lbuf[g, :, 0:t], lse_rows)
    lse_cols = dot_exact(lse_rows, eye8, first)
    lses = []
    for g in range(grp):
        stats = obl[g].astype(f32)
        lses.append(
            (stats[:, 0:1] + stats[:, 1:2] + stats[:, 2:3], lse_cols[:, g : g + 1])
        )
    top_a = functools.reduce(jnp.maximum, [v[0] for v in lses])
    top_b = functools.reduce(jnp.maximum, [v[1] for v in lses])
    sum_a, sum_b = 0.0, 0.0
    acc_a, acc_b = 0.0, 0.0
    for g in range(grp):
        wa = jnp.exp2(lses[g][0] - top_a)
        wb = jnp.exp2(lses[g][1] - top_b)
        sum_a, sum_b = sum_a + wa, sum_b + wb
        acc_a = acc_a + wa * obl[g].astype(f32)
        acc_b = acc_b + wb * obb[g].astype(f32)
    head_a = jnp.where(lane_a >= HA, acc_a / sum_a, 0.0).astype(bf16)
    head_b = (acc_b / sum_b).astype(bf16)
    msend[:, 0:128] = head_a
    msend[:, 128:256] = head_b
    pick_a = (row8 == 0).astype(f32)
    pick_b = (row8 == 1).astype(f32)
    sq_a, sq_b = head_a.astype(f32), head_b.astype(f32)
    stsend[...] = jnp.zeros_like(stsend)
    squares = dot_exact(pick_a, sq_a * sq_a, last) + dot_exact(pick_b, sq_b * sq_b, last)
    stsend[:, 0:t] = squares[0:2]
    for d in range(1, ntp):
        n = (tp + d) % ntp
        send(stsend, stbuf.at[tp], st_s.at[d], st_r.at[tp], tp_dev(n))
    stbuf[tp] = stsend[...]
    for d in range(1, nx):
        to = (x + d) % nx
        send(msend, mbuf.at[x], m_s.at[d], m_r.at[x], (z, c, y, to))
    mbuf[x] = msend[...]
    for d in range(1, ntp):
        n = (tp + d) % ntp
        landed(stbuf.at[n], st_r.at[n])
    sums = jnp.sum(stbuf[...], axis=0)[:, 0:t]
    row_t = lax.broadcasted_iota(jnp.int32, (8, t), 0)
    sums = jnp.where(row_t == 0, sums[0:1] * (1.0 / (ntp * HA)), sums[1:2] * (1.0 / (ntp * HB)))
    inverse = lax.rsqrt(sums + epsilon)
    norm_a = dot_exact(inverse, pick_a, first)
    norm_b = dot_exact(inverse, pick_b, first)
    for d in range(1, nx):
        n = (x + d) % nx
        landed(mbuf.at[n], m_r.at[n])
    for copy in locals_:
        copy.wait()
    for d in range(1, ny):
        n = (y + d) % ny
        landed(wo.at[n, :, 1], wo_r.at[0, n])
        landed(wo.at[n, :, pl.ds(2, 2)], wo_r.at[1, n])
    for n in range(nx):
        gain = mg_ref[pl.ds((y * nx + n) // 2, 1)]
        if n % 2 == 0:
            gain = pltpu.roll(gain, HA, 1)
        part = mbuf[n]
        mbuf[n, :, 0:128] = (part[:, 0:128].astype(f32) * norm_a * gain).astype(bf16)
        gain = mg_ref[pl.ds(ntp // 2 + y * nx + n, 1)]
        mbuf[n, :, 128:256] = (part[:, 128:256].astype(f32) * norm_b * gain).astype(bf16)

    def project(n):
        acc = dot_n(mbuf[0], wo[n, 0].reshape(FW, FW))
        for m in range(1, nx):
            acc = acc + dot_n(mbuf[m], wo[n, m].reshape(FW, FW))
        return acc

    for d in range(1, ny):
        to = (y + d) % ny
        psend[d] = project(to).astype(bf16)
        send(psend.at[d], pbuf.at[y], p_s.at[d], p_r.at[y], (z, c, to, x))
    for d in range(1, nx):
        if d not in near_x:
            send_up(d)
    total = tok_ref[...].astype(f32) + project(y)
    for d in range(1, ny):
        n = (y + d) % ny
        landed(pbuf.at[n], p_r.at[n])
        total = total + pbuf[n].astype(f32)
    stream[...] = total
    ones8 = jnp.ones((8, FW), f32)
    st2send[...] = jnp.zeros_like(st2send)
    st2send[:, 0:t] = dot_exact(ones8, total * total, last)[0:1]
    for d in range(1, ntp):
        n = (tp + d) % ntp
        send(st2send, st2buf.at[tp], st2_s.at[d], st2_r.at[tp], tp_dev(n))
    st2buf[tp] = st2send[...]

    feats = (total * cg_ref[...]).astype(bf16)
    picked = dot_n(sel0[...] + sel1[...], feats).astype(bf16)
    for n in range(nsp):
        outgo[n] = picked[n * cap : (n + 1) * cap]
    near = s // cb

    def dispatch(n):
        copy = rcopy(outgo.at[n], xbuf.at[y, s], d_s.at[n], d_r.at[s], sp_dev(n))
        copy.start()
        return copy

    def dispatch_far(far):
        for i in range(cb):
            for d in sorted({NCH - far, far}, reverse=True):
                sends.append(dispatch((near + d) % NCH * cb + i))

    for copy in [dispatch(near * cb + (s + d) % cb) for d in range(1, cb)]:
        copy.wait_send()
    xbuf[y, s] = outgo[s]
    for far in range(1, NCH // 2):
        dispatch_far(far)
    for d in range(1, ntp):
        n = (tp + d) % ntp
        landed(st2buf.at[n], st2_r.at[n])
    squares = jnp.sum(st2buf[...], axis=0)[:, 0:t]
    inverse = lax.rsqrt(squares * (1.0 / (ntp * FW)) + epsilon)
    inverse = jnp.broadcast_to(inverse, (8, t))
    parts = split3(inverse)
    split = jnp.where(row_t == 0, parts[0], jnp.where(row_t == 1, parts[1], parts[2]))
    split = jnp.where(row_t < 3, split, 0.0).astype(bf16)
    factors = jnp.sum(dot_t(split, sel_wide[...]), axis=0, keepdims=True)
    for n in range(nsp // per):
        scsend[n] = factors[:, n * 128 : (n + 1) * 128]
    for d in range(1, nsp):
        n = (s + d) % nsp
        send(scsend.at[n // per], scbuf.at[s], sc_s.at[d], sc_r.at[s], sp_dev(n))
    scbuf[s] = scsend[s // per]
    dispatch_far(NCH // 2)

    def chunk(k):
        return (near + NCH + (k + 1) // 2 * (2 * (k % 2) - 1)) % NCH

    def stage_a(k):
        ch = chunk(k)
        for i in range(cb):
            b = ch * cb + i

            @pl.when(b != s)
            def _():
                landed(xbuf.at[y, b], d_r.at[b])

        part = xbuf.at[y, pl.ds(ch * cb, cb)]
        for d in range(1, ny):
            to = (y + d) % ny
            rcopy(part, part, ya_s.at[ch, d], ya_r.at[ch, y], (z, c, to, x)).start()

    def stage_b(k):
        ch = chunk(k)
        for d in range(1, ny):
            n = (y + d) % ny
            landed(xbuf.at[n, pl.ds(ch * cb, cb)], ya_r.at[ch, n])

        @pl.when(k == 0)
        def _():
            for d in range(1, nx):
                n = (x + d) % nx
                landed(wgu.at[n, :, :, pl.ds(0, FE)], wg_r.at[0, n])
                landed(wgu.at[n, :, :, pl.ds(FE, FE)], wg_r.at[1, n])

        xs = [xbuf[n, pl.ds(ch * cb, cb)].reshape(rows, FW) for n in range(ny)]

        def expand(n):
            acc = dot_n(xs[0], wgu[n, 0])
            for m in range(1, ny):
                acc = acc + dot_n(xs[m], wgu[n, m])
            return acc

        for d in range(1, nx):
            to = (x + d) % nx
            rsend[ch, d] = expand(to).astype(bf16)
            rcopy(
                rsend.at[ch, d], rbuf.at[ch, x], rx_s.at[ch, d], rx_r.at[ch, x], (z, c, y, to)
            ).start()
        gown[ch] = expand(x)

    def stage_c(k):
        ch = chunk(k)
        both = gown[ch]
        for d in range(1, nx):
            n = (x + d) % nx
            landed(rbuf.at[ch, n], rx_r.at[ch, n])
            both = both + rbuf[ch, n].astype(f32)
        row = lax.broadcasted_iota(jnp.int32, (cap, 128), 0)
        spot = row + s % per * wide == lax.broadcasted_iota(jnp.int32, (cap, 128), 1)
        factor = []
        for i in range(cb):
            b = ch * cb + i

            @pl.when(b != s)
            def _():
                landed(scbuf.at[b], sc_r.at[b])

            value = jnp.where(spot, scbuf[b], 0.0)
            factor.append(jnp.sum(value, axis=1, keepdims=True))
        both = both * jnp.concatenate(factor, axis=0)
        gate_value = both[:, 0:FE]
        hidden = (gate_value / (1.0 + jnp.exp(-gate_value)) * both[:, FE:]).astype(bf16)
        hbuf[ch, x] = hidden
        for d in range(1, nx):
            to = (x + d) % nx
            rcopy(
                hbuf.at[ch, x], hbuf.at[ch, x], hx_s.at[ch, d], hx_r.at[ch, x], (z, c, y, to)
            ).start()

    def stage_d(k):
        ch = chunk(k)
        for d in range(1, nx):
            n = (x + d) % nx
            landed(hbuf.at[ch, n], hx_r.at[ch, n])

        @pl.when(k == 0)
        def _():
            for d in range(1, ny):
                n = (y + d) % ny
                landed(wd.at[n], wd_r.at[n])

        wide = jnp.concatenate([hbuf[ch, n] for n in range(nx)], axis=1)
        for d in range(1, ny):
            to = (y + d) % ny
            dsend[ch, d] = dot_n(wide, wd[to]).astype(bf16)
            rcopy(
                dsend.at[ch, d], dbuf.at[ch, y], ry_s.at[ch, d], ry_r.at[ch, y], (z, c, to, x)
            ).start()
        down_own[ch] = dot_n(wide, wd[y])

    def stage_e(k):
        ch = chunk(k)
        acc = down_own[ch]
        for d in range(1, ny):
            n = (y + d) % ny
            landed(dbuf.at[ch, n], ry_r.at[ch, n])
            acc = acc + dbuf[ch, n].astype(f32)
        eout[pl.ds(ch * cb, cb)] = acc.astype(bf16).reshape(cb, cap, FW)
        for i in range(cb):
            b = ch * cb + i

            @pl.when(b != s)
            def _():
                rcopy(eout.at[b], ret.at[s], b_s.at[b], b_r.at[s], sp_dev(b)).start()

            @pl.when(b == s)
            def _():
                ret[s] = eout[b]


    stages = (stage_a, stage_b, stage_c, stage_d, stage_e)

    ahead = ((1, 1), (1, 2)) if NCH == 4 else ()
    behind = ((0, 0), (2, 3)) if NCH == 4 else tuple((k, k) for k in range(NCH))

    def step(i, carry):
        for at, k in ahead:

            @pl.when(i == at)
            def _():
                stage_a(k)

        for lag in (4, 3, 2, 1):

            @pl.when((i >= lag) & (i < NCH + lag))
            def _():
                stages[lag](i - lag)

        for at, k in behind:

            @pl.when(i == at)
            def _():
                stage_a(k)

        return carry

    lax.fori_loop(0, NCH + len(stages) - 1, step, 0)

    for d in range(1, nsp):
        n = (s + d) % nsp
        landed(ret.at[n], b_r.at[n])
    back = ret[...].reshape(nsp * cap, FW)
    gap = rl_ref[0:1] - rl_ref[1:2]
    w0 = gw_ref[...] / (1.0 + jnp.exp(-gap))
    w1 = gw_ref[...] / (1.0 + jnp.exp(gap))
    both = jnp.where(row_t == 0, w0, jnp.where(row_t == 1, w1, 0.0))
    w0, w1 = dot_exact(both, pick_a, first), dot_exact(both, pick_b, first)
    w0, w1 = jnp.concatenate([w0, w0], axis=1), jnp.concatenate([w1, w1], axis=1)
    routed = w0 * flipped(sel0[...], back) + w1 * flipped(sel1[...], back)
    o_ref[...] = (stream[...] + routed).astype(bf16)

    for copy in sends:
        copy.wait_send()

    for part, (src, dst) in enumerate(kv_pairs):

        @pl.when(source)
        def _():
            for n in (*range(len(hubs)), nz - 1):
                landed(src, kv_s.at[part, n])

        for i in range(nb):
            relay = (c == i % 2) & (z != (i * grp + j) // 2)

            @pl.when(relay)
            def _():
                landed(dst.at[i], kv_f.at[part, i, 0])

            @pl.when(hub(i))
            def _():
                for n in (1, 2):
                    landed(dst.at[i], kv_f.at[part, i, n])

    for d in range(1, grp):
        g = (j + d) % grp
        landed(osl.at[g], o_s.at[0, g])
        landed(osb.at[g], o_s.at[1, g])
    for ch in range(NCH):
        for d in range(1, ny):
            landed(xbuf.at[y, pl.ds(ch * cb, cb)], ya_s.at[ch, d])
            landed(dsend.at[ch, d], ry_s.at[ch, d])
        for d in range(1, nx):
            landed(rsend.at[ch, d], rx_s.at[ch, d])
            landed(hbuf.at[ch, x], hx_s.at[ch, d])
    for d in range(1, nsp):
        b = (s + d) % nsp
        landed(eout.at[b], b_s.at[b])


def on_device(
    tokens,
    lean_query,
    lean_key,
    lean_value,
    lean_gains,
    broad_query,
    broad_key,
    broad_value,
    broad_gains,
    mixer_gain,
    output_weight,
    channel_gain,
    gate_weight,
    up_weight,
    down_weight,
    route_experts,
    route_logits,
    group_weight,
):
    nz, ny, nx = lax.axis_size("z"), lax.axis_size("y"), lax.axis_size("x")
    nsp, ntp = nz * 2, ny * nx
    t = tokens.shape[0]
    cap = t // (nsp // GROUPS)
    wide = 32 if cap <= 32 else 128
    half = ny // KV
    grp = nx
    nb = nsp // grp
    cb = nsp // NCH
    rows = cb * cap
    bf16, f32 = jnp.bfloat16, jnp.float32
    vm = pl.BlockSpec(memory_space=pltpu.VMEM)
    hbm = pl.BlockSpec(memory_space=pl.ANY)
    dma = pltpu.SemaphoreType.DMA
    return pl.pallas_call(
        functools.partial(layer_kernel, (nz, ny, nx, t, cap)),
        out_shape=jax.ShapeDtypeStruct((t, FW), bf16),
        in_specs=[vm] * 9 + [hbm] * 5 + [vm] * 5,
        out_specs=vm,
        scratch_shapes=[
            pltpu.VMEM((t, 256), bf16),
            pltpu.VMEM((t, 128), bf16),
            pltpu.VMEM((t, 256), bf16),
            pltpu.VMEM((grp, t, 256), bf16),
            pltpu.VMEM((nb, t, 128), bf16),
            pltpu.VMEM((nb, t, 256), bf16),
            pltpu.VMEM((grp, t, 128), bf16),
            pltpu.VMEM((grp, t, 128), bf16),
            pltpu.VMEM((grp, t, 128), bf16),
            pltpu.VMEM((grp, t, 128), bf16),
            pltpu.VMEM((8, 1, 256), f32),
            pltpu.VMEM((grp, 1, 256), f32),
            pltpu.VMEM((ny, nx, 4, 64, FW), bf16),
            pltpu.VMEM((nx, ny, FW, FW), bf16),
            pltpu.VMEM((ny, nx * FE, FW), bf16),
            pltpu.VMEM((t, 256), bf16),
            pltpu.VMEM((nx, t, 256), bf16),
            pltpu.VMEM((2, 256), f32),
            pltpu.VMEM((ntp, 2, 256), f32),
            pltpu.VMEM((ny, t, FW), bf16),
            pltpu.VMEM((ny, t, FW), bf16),
            pltpu.VMEM((1, 256), f32),
            pltpu.VMEM((ntp, 1, 256), f32),
            pltpu.VMEM((t, FW), f32),
            pltpu.VMEM((nsp * cap, t), bf16),
            pltpu.VMEM((nsp * cap, t), bf16),
            pltpu.VMEM((nsp * wide, t), bf16),
            pltpu.VMEM((nsp * wide // 128, 1, 128), f32),
            pltpu.VMEM((nsp, 1, 128), f32),
            pltpu.VMEM((nsp, cap, FW), bf16),
            pltpu.VMEM((ny, nsp, cap, FW), bf16),
            pltpu.VMEM((NCH, nx, rows, FW), bf16),
            pltpu.VMEM((NCH, nx, rows, FW), bf16),
            pltpu.VMEM((NCH, rows, FW), f32),
            pltpu.VMEM((NCH, nx, rows, FE), bf16),
            pltpu.VMEM((NCH, ny, rows, FW), bf16),
            pltpu.VMEM((NCH, ny, rows, FW), bf16),
            pltpu.VMEM((NCH, rows, FW), f32),
            pltpu.VMEM((nsp, cap, FW), bf16),
            pltpu.VMEM((nsp, cap, FW), bf16),
            dma((grp,)),
            dma((grp,)),
            dma((2, nz)),
            dma((2, nb)),
            dma((2, nb, 3)),
            dma((3, grp)),
            dma((3, grp)),
            dma((2, ny)),
            dma((2, ny)),
            dma((2, nx)),
            dma((2, nx)),
            dma((ny,)),
            dma((ny,)),
            dma((5,)),
            dma((nx,)),
            dma((nx,)),
            dma((ntp,)),
            dma((ntp,)),
            dma((ny,)),
            dma((ny,)),
            dma((ntp,)),
            dma((ntp,)),
            dma((nsp,)),
            dma((nsp,)),
            dma((nsp,)),
            dma((nsp,)),
            dma((NCH, ny)),
            dma((NCH, ny)),
            dma((NCH, nx)),
            dma((NCH, nx)),
            dma((NCH, nx)),
            dma((NCH, nx)),
            dma((NCH, ny)),
            dma((NCH, ny)),
            dma((nsp,)),
            dma((nsp,)),
        ],
        compiler_params=pltpu.CompilerParams(
            collective_id=0, has_side_effects=True, vmem_limit_bytes=60 * 1024 * 1024
        ),
    )(
        lean_query.transpose(1, 2, 0)[0],
        lean_key.transpose(1, 2, 0),
        lean_value.transpose(1, 2, 0),
        lean_gains,
        broad_query[:, 0],
        broad_key.reshape(KV * t, HB),
        broad_value.reshape(KV * t, HB),
        broad_gains,
        tokens,
        output_weight.reshape(3 * ntp, 64, FW),
        output_weight.reshape(3 * ntp // 2, 2, 64, FW),
        gate_weight.reshape(ny, nx, FW, FE),
        up_weight.reshape(ny, nx, FW, FE),
        down_weight.reshape(ny, nx * FE, FW),
        mixer_gain.reshape(-1, 128),
        channel_gain.reshape(1, FW),
        route_experts.T,
        route_logits.T,
        group_weight.reshape(1, t),
    )


def solution(mesh):
    finer = Mesh(
        mesh.devices.reshape(mesh.shape["sp"] // 2, 2, NY, NX), ("z", "c", "y", "x")
    )
    sp, tp = ("z", "c"), ("y", "x")
    return jax.shard_map(
        on_device,
        mesh=finer,
        in_specs=(
            P(sp, tp),
            P(sp, tp, None),
            P(sp, None, None),
            P(sp, None, None),
            P(),
            P(sp, tp, None),
            P(sp, None, None),
            P(sp, None, None),
            P(),
            P(),
            P(None, tp),
            P(tp),
            P(sp, None, tp),
            P(sp, None, tp),
            P(sp, None, tp),
            P(sp, None),
            P(sp, None),
            P(sp),
        ),
        out_specs=P(sp, tp),
        check_vma=False,
    )
```

```python
import functools
import math

import jax
import jax.numpy as jnp
from jax import lax
from jax.experimental import pallas as pl
from jax.experimental.pallas import tpu as pltpu
from jax.sharding import Mesh
from jax.sharding import PartitionSpec as P

D = 4096
GRID_W = 64
GRID_BITS = 6
KV = 2
GROUPS = 4
NY, NX = 4, 4
NCH = 4
HUBS = (8, 5, 11, 2, 14)
UNROLL = 2
HA, HB = 64, 128
FW = 256
FE = 128
MESH = pl.DeviceIdType.MESH
epsilon = 1e-06
theta_base = 10000.0
LOG2E = 1.4426950408889634


def rcopy(src, dst, send_sem, recv_sem, device):
    return pltpu.make_async_remote_copy(
        src_ref=src,
        dst_ref=dst,
        send_sem=send_sem,
        recv_sem=recv_sem,
        device_id=device,
        device_id_type=MESH,
    )


def landed(ref, sem):
    pltpu.make_async_copy(ref, ref, sem).wait()


def dot_t(a, b):
    return lax.dot_general(a, b, (((1,), (1,)), ((), ())), preferred_element_type=jnp.float32)


def dot_n(a, b):
    return jnp.dot(a, b, preferred_element_type=jnp.float32)


def dot_exact(a, b, dims):
    return lax.dot_general(
        a,
        b,
        (dims, ((), ())),
        preferred_element_type=jnp.float32,
        precision=lax.Precision.HIGHEST,
    )


def layer_kernel(
    dims,
    lq_ref,
    lk_ref,
    lv_ref,
    lg_ref,
    bq_ref,
    bk_ref,
    bv_ref,
    bg_ref,
    tok_ref,
    wl_ref,
    wb_ref,
    gate_ref,
    up_ref,
    down_ref,
    mg_ref,
    cg_ref,
    re_ref,
    rl_ref,
    gw_ref,
    o_ref,
    q_ref,
    kvl_ref,
    kvb_ref,
    qbuf,
    kvl,
    kvb,
    osl,
    osb,
    obl,
    obb,
    lsend,
    lbuf,
    wo,
    wgu,
    wd,
    msend,
    mbuf,
    stsend,
    stbuf,
    psend,
    pbuf,
    st2send,
    st2buf,
    stream,
    sel0,
    sel1,
    sel_wide,
    scsend,
    scbuf,
    outgo,
    xbuf,
    rsend,
    rbuf,
    gown,
    hbuf,
    dsend,
    dbuf,
    down_own,
    eout,
    ret,
    q_s,
    q_r,
    kv_s,
    kv_r,
    kv_f,
    o_s,
    o_r,
    wo_s,
    wo_r,
    wg_s,
    wg_r,
    wd_s,
    wd_r,
    loc,
    m_s,
    m_r,
    st_s,
    st_r,
    p_s,
    p_r,
    st2_s,
    st2_r,
    d_s,
    d_r,
    sc_s,
    sc_r,
    ya_s,
    ya_r,
    rx_s,
    rx_r,
    hx_s,
    hx_r,
    ry_s,
    ry_r,
    b_s,
    b_r,
):
    nz, ny, nx, t, cap = dims
    nsp = nz * 2
    ntp = ny * nx
    half = ny // KV
    grp = nx
    nb = nsp // grp
    cb = nsp // NCH
    rows = cb * cap
    wide = 32 if cap <= 32 else 128
    per = 128 // wide
    z, c = lax.axis_index("z"), lax.axis_index("c")
    y, x = lax.axis_index("y"), lax.axis_index("x")
    s = z * 2 + c
    tp = y * nx + x
    head = y // half
    j = x
    bf16, f32 = jnp.bfloat16, jnp.float32

    def member(g):
        return (z, c, y, g)

    def tp_dev(n):
        return (z, c, n // nx, n % nx)

    def sp_dev(n):
        return (n // 2, n % 2, y, x)

    barrier = pltpu.get_barrier_semaphore()
    for d in range(1, nsp):
        pl.semaphore_signal(barrier, inc=1, device_id=sp_dev((s + d) % nsp), device_id_type=MESH)
    for d in range(1, ntp):
        pl.semaphore_signal(barrier, inc=1, device_id=tp_dev((tp + d) % ntp), device_id_type=MESH)

    def turned(raw, swapped, gain, size):
        quarter = size // 4
        lane = lax.broadcasted_iota(jnp.int32, (t, 128), 1)
        at = lax.broadcasted_iota(jnp.int32, (t, 128), 0) + s * t
        spot = jnp.where(lane < size // 2, at >> GRID_BITS, at & (GRID_W - 1)).astype(f32)
        step = (lane & (quarter - 1)).astype(f32) * (-math.log(theta_base) / quarter)
        angle = spot * jnp.exp(step)
        cosine = jnp.cos(angle)
        sine = jnp.where((lane & quarter) == 0, -1.0, 1.0) * jnp.sin(angle)
        results = []
        for (a, b), (g, h) in zip(zip(raw, swapped), gain):
            scale = lax.rsqrt(jnp.sum(a * a, axis=1, keepdims=True) * (1.0 / size) + epsilon)
            results.append(scale * (a * (g * cosine) + b * (h * sine)))
        return results

    def unit(size, shift):
        row = lax.broadcasted_iota(jnp.int32, (size, 128), 0)
        lane = lax.broadcasted_iota(jnp.int32, (size, 128), 1)
        return row + shift == lane, row == (lane ^ (size // 4))

    def gain_pair(ref, swap):
        pairs = dot_exact(ref[...], swap, ((1,), (0,)))
        return pairs[0:1], pairs[1:2]

    first = ((0,), (0,))

    def flipped(array, matrix):
        return lax.dot_general(array, matrix, (first, ((), ())), preferred_element_type=f32)

    same, swap = unit(HA, 0)
    place, _ = unit(HA, HA)
    same_b, swap_b, place_b = same.astype(bf16), swap.astype(bf16), place.astype(bf16)
    lk = lk_ref[head]
    g_raw, g_swap = gain_pair(lg_ref, same.astype(f32)), gain_pair(lg_ref, swap.astype(f32))
    q_a, k_a = turned(
        (flipped(lq_ref[...], same_b), flipped(lk, same_b)),
        (flipped(lq_ref[...], swap_b), flipped(lk, swap_b)),
        tuple(zip(g_raw, g_swap)),
        HA,
    )
    q_ref[:, 0:128] = q_a.astype(bf16)
    kvl_ref[...] = (k_a + flipped(lv_ref[head], place_b)).astype(bf16)
    _, swap = unit(HB, 0)
    swap_b = swap.astype(bf16)
    pair_row = lax.broadcasted_iota(jnp.int32, (t, KV * t), 0) * KV + head
    pick = (pair_row == lax.broadcasted_iota(jnp.int32, (t, KV * t), 1)).astype(bf16)
    k_raw = dot_n(pick, bk_ref[...])
    g_raw = (bg_ref[0:1], bg_ref[1:2])
    q_b, k_b = turned(
        (bq_ref[...].astype(f32), k_raw),
        (dot_n(bq_ref[...], swap_b), dot_n(k_raw.astype(bf16), swap_b)),
        tuple(zip(g_raw, gain_pair(bg_ref, swap.astype(f32)))),
        HB,
    )
    q_ref[:, 128:256] = q_b.astype(bf16)
    kvb_ref[:, 0:128] = k_b.astype(bf16)
    kvb_ref[:, 128:256] = dot_n(pick, bv_ref[...]).astype(bf16)

    experts = lax.broadcasted_iota(jnp.int32, (nsp, t), 0)
    e0 = (experts == re_ref[0:1]).astype(f32)
    e1 = (experts == re_ref[1:2]).astype(f32)
    before = (
        lax.broadcasted_iota(jnp.int32, (t, t), 0) < lax.broadcasted_iota(jnp.int32, (t, t), 1)
    ).astype(bf16)
    rank = dot_n((e0 + e1).astype(bf16), before)

    def slots(pitch):
        row = lax.broadcasted_iota(jnp.int32, (nsp * pitch, t), 0)
        place = rank + (experts * pitch).astype(f32)
        for e in (e0, e1):
            slot = jnp.sum(e * place, axis=0, keepdims=True).astype(jnp.int32)
            yield (row == slot).astype(f32)

    for part, sel in zip(slots(cap), (sel0, sel1)):
        sel[...] = part.astype(bf16)
    sel_wide[...] = sum(slots(wide)).astype(bf16)
    wo[:, :, 0] = jnp.zeros_like(wo[:, :, 0])
    qbuf[j] = q_ref[...]

    pl.semaphore_wait(barrier, nsp - 1 + ntp - 1)

    def send(src, dst, send_sem, recv_sem, device):
        copy = rcopy(src, dst, send_sem, recv_sem, device)
        copy.start()

    source = s % grp == j
    mine = s // grp
    hubs = HUBS if nz == 16 else tuple(range(1, nz))
    kv_pairs = ((kvl_ref, kvl), (kvb_ref, kvb))

    @pl.when(source)
    def _():
        for part, (src, dst) in enumerate(kv_pairs):
            for n, d in enumerate(hubs):
                rcopy(
                    src,
                    dst.at[mine],
                    kv_s.at[part],
                    kv_r.at[part, mine],
                    ((z + d) % nz, mine % 2, y, x),
                ).start()
            rcopy(
                src, dst.at[mine], kv_s.at[part], kv_r.at[part, mine], (z, 1 - c, y, x)
            ).start()

    for d in range(1, grp):
        g = (j + d) % grp
        send(q_ref, qbuf.at[j], q_s.at[0], q_r.at[0], member(g))

    locals_ = []

    def local(src, dst, n):
        copy = pltpu.make_async_copy(src, dst, loc.at[n])
        copy.start()
        locals_.append(copy)

    local(wl_ref.at[pl.ds(y * nx, nx)], wo.at[y, :, 1], 0)
    local(wb_ref.at[pl.ds(ntp // 2 + y * nx, nx)], wo.at[y, :, pl.ds(2, 2)], 1)
    local(gate_ref.at[:, x], wgu.at[x, :, :, pl.ds(0, FE)], 2)
    for d in range(1, ny):
        to = (y + d) % ny
        dev = (z, c, to, x)
        send(wl_ref.at[pl.ds(to * nx, nx)], wo.at[y, :, 1], wo_s.at[0], wo_r.at[0], dev)
        send(
            wb_ref.at[pl.ds(ntp // 2 + to * nx, nx)],
            wo.at[y, :, pl.ds(2, 2)],
            wo_s.at[1],
            wo_r.at[1],
            dev,
        )
    for d in range(1, nx):
        to = (x + d) % nx
        dev = (z, c, y, to)
        send(gate_ref.at[:, to], wgu.at[x, :, :, pl.ds(0, FE)], wg_s.at[0], wg_r.at[0], dev)

    def send_up(d):
        to = (x + d) % nx
        dev = (z, c, y, to)
        send(up_ref.at[:, to], wgu.at[x, :, :, pl.ds(FE, FE)], wg_s.at[1], wg_r.at[1], dev)

    near_x = sorted({1, nx - 1})
    for d in near_x:
        send_up(d)

    for d in range(1, ny):
        to = (y + d) % ny
        send(down_ref.at[to], wd.at[y], wd_s.at[0], wd_r.at[0], (z, c, to, x))

    local(up_ref.at[:, x], wgu.at[x, :, :, pl.ds(FE, FE)], 3)
    local(down_ref.at[y], wd.at[y], 4)

    def away(i):
        return (z - (i * grp + j) // 2 + nz) % nz

    def hub(i):
        return (c == i % 2) & (away(i) % 3 == 2) if nz == 16 else away(i) < 0

    def pass_on(part, i):
        dst = kv_pairs[part][1]
        landed(dst.at[i], kv_r.at[part, i])

        @pl.when((c == i % 2) & (away(i) != 0))
        def _():
            rcopy(
                dst.at[i], dst.at[i], kv_f.at[part, i], kv_r.at[part, i], (z, 1 - c, y, x)
            ).start()

    def arrive_first(part):
        src, dst = kv_pairs[part]
        for i in range(nb):

            @pl.when((mine == i) & source)
            def _():
                dst[i] = src[...]

            @pl.when(hub(i))
            def _():
                pass_on(part, i)
                for d in (1, nz - 1):
                    rcopy(
                        dst.at[i],
                        dst.at[i],
                        kv_f.at[part, i],
                        kv_r.at[part, i],
                        ((z + d) % nz, c, y, x),
                    ).start()

    def arrive(part):
        for i in range(nb):
            direct = ((mine == i) & source) | hub(i)

            @pl.when(jnp.logical_not(direct))
            def _():
                pass_on(part, i)

    arrive_first(0)
    arrive(0)
    arrive_first(1)
    landed(qbuf.at[pl.ds(0, grp - 1)], q_r.at[0])

    scale_a = HA**-0.5 * LOG2E
    scale_b = HB**-0.5 * LOG2E
    lane_a = lax.broadcasted_iota(jnp.int32, (t, 128), 1)

    def attend(scores, values, scale):
        peak = jnp.max(scores, axis=1, keepdims=True) * scale
        weights = jnp.exp2(scores * scale - peak)
        total = jnp.sum(weights, axis=1, keepdims=True)
        out = dot_n(weights.astype(bf16), values) / total
        return out, peak + jnp.log(total) * LOG2E

    def split3(v):
        a = v.astype(bf16).astype(f32)
        b = (v - a).astype(bf16).astype(f32)
        return a, b, v - a - b

    def marked(value, lse, at):
        for n, piece in enumerate(split3(lse)):
            value = jnp.where(lane_a == at + n, piece, value)
        return value

    def hand_over(part, src, dst, d, g):
        @pl.when(d < grp)
        def _():
            rcopy(src.at[g], dst.at[j], o_s.at[part], o_r.at[part], member(g)).start()

        @pl.when(d == grp)
        def _():
            dst[j] = src[g]

    def lean_head(d, carry):
        g = (j + d) % grp
        kv_l = kvl[...].reshape(nb * t, 128)
        out, lse = attend(dot_t(qbuf[g, :, 0:128], kv_l), kv_l, scale_a)
        osl[g] = marked(out, lse, 0).astype(bf16)
        hand_over(0, osl, obl, d, g)
        return carry

    def broad_head(d, lses):
        g = (j + d) % grp
        k_b = kvb[:, :, 0:128].reshape(nb * t, 128)
        v_b = kvb[:, :, 128:256].reshape(nb * t, 128)
        out, lse = attend(dot_t(qbuf[g, :, 128:256], k_b), v_b, scale_b)
        osb[g] = out.astype(bf16)
        hand_over(1, osb, obb, d, g)
        return jnp.where(lane_a == g, lse, lses)

    lax.fori_loop(1, grp + 1, lean_head, 0, unroll=UNROLL)
    arrive(1)
    lses = lax.fori_loop(1, grp + 1, broad_head, jnp.zeros((t, 128), f32), unroll=UNROLL)
    last = ((1,), (1,))
    row8 = lax.broadcasted_iota(jnp.int32, (8, 128), 0)
    eye8 = (row8 == lax.broadcasted_iota(jnp.int32, (8, 128), 1)).astype(f32)
    lsend[...] = jnp.zeros_like(lsend)
    lse_rows = dot_exact(eye8, lses, last)
    for g in range(grp):
        lsend[g, :, 0:t] = lse_rows[g : g + 1]
    for d in range(1, grp):
        g = (j + d) % grp
        send(lsend.at[g], lbuf.at[j], o_s.at[2], o_r.at[2], member(g))
    lbuf[j] = lsend[j]

    landed(obl.at[pl.ds(0, grp - 1)], o_r.at[0])
    landed(obb.at[pl.ds(0, grp - 1)], o_r.at[1])
    landed(lbuf.at[pl.ds(0, grp - 1)], o_r.at[2])

    row_g = lax.broadcasted_iota(jnp.int32, (8, t), 0)
    lse_rows = jnp.zeros((8, t), f32)
    for g in range(grp):
        lse_rows = jnp.where(row_g == g, lbuf[g, :, 0:t], lse_rows)
    lse_cols = dot_exact(lse_rows, eye8, first)
    lses = []
    for g in range(grp):
        stats = obl[g].astype(f32)
        lses.append(
            (stats[:, 0:1] + stats[:, 1:2] + stats[:, 2:3], lse_cols[:, g : g + 1])
        )
    top_a = functools.reduce(jnp.maximum, [v[0] for v in lses])
    top_b = functools.reduce(jnp.maximum, [v[1] for v in lses])
    sum_a, sum_b = 0.0, 0.0
    acc_a, acc_b = 0.0, 0.0
    for g in range(grp):
        wa = jnp.exp2(lses[g][0] - top_a)
        wb = jnp.exp2(lses[g][1] - top_b)
        sum_a, sum_b = sum_a + wa, sum_b + wb
        acc_a = acc_a + wa * obl[g].astype(f32)
        acc_b = acc_b + wb * obb[g].astype(f32)
    head_a = jnp.where(lane_a >= HA, acc_a / sum_a, 0.0).astype(bf16)
    head_b = (acc_b / sum_b).astype(bf16)
    msend[:, 0:128] = head_a
    msend[:, 128:256] = head_b
    pick_a = (row8 == 0).astype(f32)
    pick_b = (row8 == 1).astype(f32)
    sq_a, sq_b = head_a.astype(f32), head_b.astype(f32)
    stsend[...] = jnp.zeros_like(stsend)
    squares = dot_exact(pick_a, sq_a * sq_a, last) + dot_exact(pick_b, sq_b * sq_b, last)
    stsend[:, 0:t] = squares[0:2]
    for d in range(1, ntp):
        n = (tp + d) % ntp
        send(stsend, stbuf.at[tp], st_s.at[0], st_r.at[0], tp_dev(n))
    stbuf[tp] = stsend[...]
    for d in range(1, nx):
        to = (x + d) % nx
        send(msend, mbuf.at[x], m_s.at[0], m_r.at[0], (z, c, y, to))
    mbuf[x] = msend[...]
    landed(stbuf.at[pl.ds(0, ntp - 1)], st_r.at[0])
    sums = jnp.sum(stbuf[...], axis=0)[:, 0:t]
    row_t = lax.broadcasted_iota(jnp.int32, (8, t), 0)
    sums = jnp.where(row_t == 0, sums[0:1] * (1.0 / (ntp * HA)), sums[1:2] * (1.0 / (ntp * HB)))
    inverse = lax.rsqrt(sums + epsilon)
    norm_a = dot_exact(inverse, pick_a, first)
    norm_b = dot_exact(inverse, pick_b, first)
    landed(mbuf.at[pl.ds(0, nx - 1)], m_r.at[0])
    for copy in locals_:
        copy.wait()
    landed(wo.at[pl.ds(0, ny - 1), :, 1], wo_r.at[0])
    landed(wo.at[pl.ds(0, ny - 1), :, pl.ds(2, 2)], wo_r.at[1])
    for n in range(nx):
        gain = mg_ref[pl.ds((y * nx + n) // 2, 1)]
        if n % 2 == 0:
            gain = pltpu.roll(gain, HA, 1)
        part = mbuf[n]
        mbuf[n, :, 0:128] = (part[:, 0:128].astype(f32) * norm_a * gain).astype(bf16)
        gain = mg_ref[pl.ds(ntp // 2 + y * nx + n, 1)]
        mbuf[n, :, 128:256] = (part[:, 128:256].astype(f32) * norm_b * gain).astype(bf16)

    def project(n):
        acc = dot_n(mbuf[0], wo[n, 0].reshape(FW, FW))
        for m in range(1, nx):
            acc = acc + dot_n(mbuf[m], wo[n, m].reshape(FW, FW))
        return acc

    for d in range(1, ny):
        to = (y + d) % ny
        psend[d] = project(to).astype(bf16)
        send(psend.at[d], pbuf.at[y], p_s.at[0], p_r.at[0], (z, c, to, x))
    for d in range(1, nx):
        if d not in near_x:
            send_up(d)
    total = tok_ref[...].astype(f32) + project(y)
    landed(pbuf.at[pl.ds(0, ny - 1)], p_r.at[0])
    for d in range(1, ny):
        n = (y + d) % ny
        total = total + pbuf[n].astype(f32)
    stream[...] = total
    ones8 = jnp.ones((8, FW), f32)
    st2send[...] = jnp.zeros_like(st2send)
    st2send[:, 0:t] = dot_exact(ones8, total * total, last)[0:1]
    for d in range(1, ntp):
        n = (tp + d) % ntp
        send(st2send, st2buf.at[tp], st2_s.at[0], st2_r.at[0], tp_dev(n))
    st2buf[tp] = st2send[...]

    feats = (total * cg_ref[...]).astype(bf16)
    picked = dot_n(sel0[...] + sel1[...], feats).astype(bf16)
    for n in range(nsp):
        outgo[n] = picked[n * cap : (n + 1) * cap]
    near = s // cb

    def dispatch(n, part):
        send(outgo.at[n], xbuf.at[y, s], d_s.at[part], d_r.at[near], sp_dev(n))

    def dispatch_far(far):
        for i in range(cb):
            for d in sorted({NCH - far, far}, reverse=True):
                dispatch((near + d) % NCH * cb + i, 1)

    for d in range(1, cb):
        dispatch(near * cb + (s + d) % cb, 0)
    landed(outgo.at[pl.ds(0, cb - 1)], d_s.at[0])
    xbuf[y, s] = outgo[s]
    for far in range(1, NCH // 2):
        dispatch_far(far)
    landed(st2buf.at[pl.ds(0, ntp - 1)], st2_r.at[0])
    squares = jnp.sum(st2buf[...], axis=0)[:, 0:t]
    inverse = lax.rsqrt(squares * (1.0 / (ntp * FW)) + epsilon)
    inverse = jnp.broadcast_to(inverse, (8, t))
    parts = split3(inverse)
    split = jnp.where(row_t == 0, parts[0], jnp.where(row_t == 1, parts[1], parts[2]))
    split = jnp.where(row_t < 3, split, 0.0).astype(bf16)
    factors = jnp.sum(dot_t(split, sel_wide[...]), axis=0, keepdims=True)
    for n in range(nsp // per):
        scsend[n] = factors[:, n * 128 : (n + 1) * 128]
    for d in range(1, nsp):
        n = (s + d) % nsp
        send(scsend.at[n // per], scbuf.at[s], sc_s.at[0], sc_r.at[near], sp_dev(n))
    scbuf[s] = scsend[s // per]
    dispatch_far(NCH // 2)

    def chunk(k):
        return (near + NCH + (k + 1) // 2 * (2 * (k % 2) - 1)) % NCH

    def stage_a(k):
        ch = chunk(k)
        landed(xbuf.at[y, pl.ds(0, cb - (k == 0))], d_r.at[ch])
        part = xbuf.at[y, pl.ds(ch * cb, cb)]
        for d in range(1, ny):
            to = (y + d) % ny
            rcopy(part, part, ya_s.at[0], ya_r.at[ch], (z, c, to, x)).start()

    def stage_b(k):
        ch = chunk(k)
        landed(xbuf.at[pl.ds(0, ny - 1), pl.ds(0, cb)], ya_r.at[ch])

        @pl.when(k == 0)
        def _():
            for n in range(2):
                landed(wgu.at[pl.ds(0, nx - 1), :, :, pl.ds(n * FE, FE)], wg_r.at[n])

        xs = [xbuf[n, pl.ds(ch * cb, cb)].reshape(rows, FW) for n in range(ny)]

        def expand(n):
            acc = dot_n(xs[0], wgu[n, 0])
            for m in range(1, ny):
                acc = acc + dot_n(xs[m], wgu[n, m])
            return acc

        for d in range(1, nx):
            to = (x + d) % nx
            rsend[ch, d] = expand(to).astype(bf16)
            rcopy(
                rsend.at[ch, d], rbuf.at[ch, x], rx_s.at[0], rx_r.at[ch], (z, c, y, to)
            ).start()
        gown[ch] = expand(x)

    def stage_c(k):
        ch = chunk(k)
        both = gown[ch]
        landed(rbuf.at[ch, pl.ds(0, nx - 1)], rx_r.at[ch])
        for d in range(1, nx):
            n = (x + d) % nx
            both = both + rbuf[ch, n].astype(f32)
        row = lax.broadcasted_iota(jnp.int32, (cap, 128), 0)
        spot = row + s % per * wide == lax.broadcasted_iota(jnp.int32, (cap, 128), 1)
        factor = []

        @pl.when(k == 0)
        def _():
            landed(scbuf.at[pl.ds(0, cb - 1)], sc_r.at[ch])

        @pl.when(k > 0)
        def _():
            landed(scbuf.at[pl.ds(0, cb)], sc_r.at[ch])

        for i in range(cb):
            b = ch * cb + i
            value = jnp.where(spot, scbuf[b], 0.0)
            factor.append(jnp.sum(value, axis=1, keepdims=True))
        both = both * jnp.concatenate(factor, axis=0)
        gate_value = both[:, 0:FE]
        hidden = (gate_value / (1.0 + jnp.exp(-gate_value)) * both[:, FE:]).astype(bf16)
        hbuf[ch, x] = hidden
        for d in range(1, nx):
            to = (x + d) % nx
            rcopy(
                hbuf.at[ch, x], hbuf.at[ch, x], hx_s.at[0], hx_r.at[ch], (z, c, y, to)
            ).start()

    def stage_d(k):
        ch = chunk(k)
        landed(hbuf.at[ch, pl.ds(0, nx - 1)], hx_r.at[ch])

        @pl.when(k == 0)
        def _():
            landed(wd.at[pl.ds(0, ny - 1)], wd_r.at[0])

        wide = jnp.concatenate([hbuf[ch, n] for n in range(nx)], axis=1)
        for d in range(1, ny):
            to = (y + d) % ny
            dsend[ch, d] = dot_n(wide, wd[to]).astype(bf16)
            rcopy(
                dsend.at[ch, d], dbuf.at[ch, y], ry_s.at[0], ry_r.at[ch], (z, c, to, x)
            ).start()
        down_own[ch] = dot_n(wide, wd[y])

    def stage_e(k):
        ch = chunk(k)
        acc = down_own[ch]
        landed(dbuf.at[ch, pl.ds(0, ny - 1)], ry_r.at[ch])
        for d in range(1, ny):
            n = (y + d) % ny
            acc = acc + dbuf[ch, n].astype(f32)
        eout[pl.ds(ch * cb, cb)] = acc.astype(bf16).reshape(cb, cap, FW)
        for i in range(cb):
            b = ch * cb + i

            @pl.when(b != s)
            def _():
                rcopy(eout.at[b], ret.at[s], b_s.at[0], b_r.at[0], sp_dev(b)).start()

            @pl.when(b == s)
            def _():
                ret[s] = eout[b]


    stages = (stage_a, stage_b, stage_c, stage_d, stage_e)

    behind = ((0, 0), (1, 1), (1, 2), (2, 3)) if NCH == 4 else tuple((k, k) for k in range(NCH))

    def step(i, carry):
        for lag in (4, 3, 2, 1):

            @pl.when((i >= lag) & (i < NCH + lag))
            def _():
                stages[lag](i - lag)

        for at, k in behind:

            @pl.when(i == at)
            def _():
                stage_a(k)

        return carry

    lax.fori_loop(0, NCH + len(stages) - 1, step, 0)

    landed(ret.at[pl.ds(0, nsp - 1)], b_r.at[0])
    back = ret[...].reshape(nsp * cap, FW)
    gap = rl_ref[0:1] - rl_ref[1:2]
    w0 = gw_ref[...] / (1.0 + jnp.exp(-gap))
    w1 = gw_ref[...] / (1.0 + jnp.exp(gap))
    both = jnp.where(row_t == 0, w0, jnp.where(row_t == 1, w1, 0.0))
    w0, w1 = dot_exact(both, pick_a, first), dot_exact(both, pick_b, first)
    w0, w1 = jnp.concatenate([w0, w0], axis=1), jnp.concatenate([w1, w1], axis=1)
    routed = w0 * flipped(sel0[...], back) + w1 * flipped(sel1[...], back)
    o_ref[...] = (stream[...] + routed).astype(bf16)


    for part, (src, dst) in enumerate(kv_pairs):

        @pl.when(source)
        def _():
            landed(dst.at[pl.ds(0, len(hubs) + 1)], kv_s.at[part])

        for i in range(nb):

            @pl.when(hub(i))
            def _():
                landed(dst.at[pl.ds(0, min(3, nb))], kv_f.at[part, i])

            @pl.when((c == i % 2) & (away(i) != 0) & jnp.logical_not(hub(i)))
            def _():
                landed(dst.at[i], kv_f.at[part, i])

    landed(qbuf.at[pl.ds(0, grp - 1)], q_s.at[0])
    for n in range(2):
        landed(((obl, obb)[n]).at[pl.ds(0, grp - 1)], o_s.at[n])
    landed(lbuf.at[pl.ds(0, grp - 1)], o_s.at[2])
    landed(wo.at[pl.ds(0, ny - 1), :, 1], wo_s.at[0])
    landed(wo.at[pl.ds(0, ny - 1), :, pl.ds(2, 2)], wo_s.at[1])
    for n in range(2):
        landed(wgu.at[pl.ds(0, nx - 1), :, :, pl.ds(n * FE, FE)], wg_s.at[n])
    landed(wd.at[pl.ds(0, ny - 1)], wd_s.at[0])
    landed(mbuf.at[pl.ds(0, nx - 1)], m_s.at[0])
    landed(stbuf.at[pl.ds(0, ntp - 1)], st_s.at[0])
    landed(pbuf.at[pl.ds(0, ny - 1)], p_s.at[0])
    landed(st2buf.at[pl.ds(0, ntp - 1)], st2_s.at[0])
    landed(outgo.at[pl.ds(0, nsp - cb)], d_s.at[1])
    landed(scbuf.at[pl.ds(0, nsp - 1)], sc_s.at[0])
    landed(xbuf.at[pl.ds(0, ny - 1)], ya_s.at[0])
    landed(rbuf.at[:, pl.ds(0, nx - 1)], rx_s.at[0])
    landed(hbuf.at[:, pl.ds(0, nx - 1)], hx_s.at[0])
    landed(dbuf.at[:, pl.ds(0, ny - 1)], ry_s.at[0])
    landed(ret.at[pl.ds(0, nsp - 1)], b_s.at[0])


def on_device(
    tokens,
    lean_query,
    lean_key,
    lean_value,
    lean_gains,
    broad_query,
    broad_key,
    broad_value,
    broad_gains,
    mixer_gain,
    output_weight,
    channel_gain,
    gate_weight,
    up_weight,
    down_weight,
    route_experts,
    route_logits,
    group_weight,
):
    nz, ny, nx = lax.axis_size("z"), lax.axis_size("y"), lax.axis_size("x")
    nsp, ntp = nz * 2, ny * nx
    t = tokens.shape[0]
    cap = t // (nsp // GROUPS)
    wide = 32 if cap <= 32 else 128
    half = ny // KV
    grp = nx
    nb = nsp // grp
    cb = nsp // NCH
    rows = cb * cap
    bf16, f32 = jnp.bfloat16, jnp.float32
    vm = pl.BlockSpec(memory_space=pltpu.VMEM)
    hbm = pl.BlockSpec(memory_space=pl.ANY)
    dma = pltpu.SemaphoreType.DMA
    return pl.pallas_call(
        functools.partial(layer_kernel, (nz, ny, nx, t, cap)),
        out_shape=jax.ShapeDtypeStruct((t, FW), bf16),
        in_specs=[vm] * 9 + [hbm] * 5 + [vm] * 5,
        out_specs=vm,
        scratch_shapes=[
            pltpu.VMEM((t, 256), bf16),
            pltpu.VMEM((t, 128), bf16),
            pltpu.VMEM((t, 256), bf16),
            pltpu.VMEM((grp, t, 256), bf16),
            pltpu.VMEM((nb, t, 128), bf16),
            pltpu.VMEM((nb, t, 256), bf16),
            pltpu.VMEM((grp, t, 128), bf16),
            pltpu.VMEM((grp, t, 128), bf16),
            pltpu.VMEM((grp, t, 128), bf16),
            pltpu.VMEM((grp, t, 128), bf16),
            pltpu.VMEM((8, 1, 256), f32),
            pltpu.VMEM((grp, 1, 256), f32),
            pltpu.VMEM((ny, nx, 4, 64, FW), bf16),
            pltpu.VMEM((nx, ny, FW, FW), bf16),
            pltpu.VMEM((ny, nx * FE, FW), bf16),
            pltpu.VMEM((t, 256), bf16),
            pltpu.VMEM((nx, t, 256), bf16),
            pltpu.VMEM((2, 256), f32),
            pltpu.VMEM((ntp, 2, 256), f32),
            pltpu.VMEM((ny, t, FW), bf16),
            pltpu.VMEM((ny, t, FW), bf16),
            pltpu.VMEM((1, 256), f32),
            pltpu.VMEM((ntp, 1, 256), f32),
            pltpu.VMEM((t, FW), f32),
            pltpu.VMEM((nsp * cap, t), bf16),
            pltpu.VMEM((nsp * cap, t), bf16),
            pltpu.VMEM((nsp * wide, t), bf16),
            pltpu.VMEM((nsp * wide // 128, 1, 128), f32),
            pltpu.VMEM((nsp, 1, 128), f32),
            pltpu.VMEM((nsp, cap, FW), bf16),
            pltpu.VMEM((ny, nsp, cap, FW), bf16),
            pltpu.VMEM((NCH, nx, rows, FW), bf16),
            pltpu.VMEM((NCH, nx, rows, FW), bf16),
            pltpu.VMEM((NCH, rows, FW), f32),
            pltpu.VMEM((NCH, nx, rows, FE), bf16),
            pltpu.VMEM((NCH, ny, rows, FW), bf16),
            pltpu.VMEM((NCH, ny, rows, FW), bf16),
            pltpu.VMEM((NCH, rows, FW), f32),
            pltpu.VMEM((nsp, cap, FW), bf16),
            pltpu.VMEM((nsp, cap, FW), bf16),
            dma((1,)),
            dma((1,)),
            dma((2,)),
            dma((2, nb)),
            dma((2, nb)),
            dma((3,)),
            dma((3,)),
            dma((2,)),
            dma((2,)),
            dma((2,)),
            dma((2,)),
            dma((1,)),
            dma((1,)),
            dma((5,)),
            dma((1,)),
            dma((1,)),
            dma((1,)),
            dma((1,)),
            dma((1,)),
            dma((1,)),
            dma((1,)),
            dma((1,)),
            dma((2,)),
            dma((NCH,)),
            dma((1,)),
            dma((NCH,)),
            dma((1,)),
            dma((NCH,)),
            dma((1,)),
            dma((NCH,)),
            dma((1,)),
            dma((NCH,)),
            dma((1,)),
            dma((NCH,)),
            dma((1,)),
            dma((1,)),
        ],
        compiler_params=pltpu.CompilerParams(
            collective_id=0, has_side_effects=True, vmem_limit_bytes=60 * 1024 * 1024
        ),
    )(
        lean_query.transpose(1, 2, 0)[0],
        lean_key.transpose(1, 2, 0),
        lean_value.transpose(1, 2, 0),
        lean_gains,
        broad_query[:, 0],
        broad_key.reshape(KV * t, HB),
        broad_value.reshape(KV * t, HB),
        broad_gains,
        tokens,
        output_weight.reshape(3 * ntp, 64, FW),
        output_weight.reshape(3 * ntp // 2, 2, 64, FW),
        gate_weight.reshape(ny, nx, FW, FE),
        up_weight.reshape(ny, nx, FW, FE),
        down_weight.reshape(ny, nx * FE, FW),
        mixer_gain.reshape(-1, 128),
        channel_gain.reshape(1, FW),
        route_experts.T,
        route_logits.T,
        group_weight.reshape(1, t),
    )


def solution(mesh):
    finer = Mesh(
        mesh.devices.reshape(mesh.shape["sp"] // 2, 2, NY, NX), ("z", "c", "y", "x")
    )
    sp, tp = ("z", "c"), ("y", "x")
    return jax.shard_map(
        on_device,
        mesh=finer,
        in_specs=(
            P(sp, tp),
            P(sp, tp, None),
            P(sp, None, None),
            P(sp, None, None),
            P(),
            P(sp, tp, None),
            P(sp, None, None),
            P(sp, None, None),
            P(),
            P(),
            P(None, tp),
            P(tp),
            P(sp, None, tp),
            P(sp, None, tp),
            P(sp, None, tp),
            P(sp, None),
            P(sp, None),
            P(sp),
        ),
        out_specs=P(sp, tp),
        check_vma=False,
    )
```

```python
import functools
import math

import jax
import jax.numpy as jnp
from jax import lax
from jax.experimental import pallas as pl
from jax.experimental.pallas import tpu as pltpu
from jax.sharding import Mesh
from jax.sharding import PartitionSpec as P

D = 4096
GRID_W = 64
GRID_BITS = 6
KV = 2
GROUPS = 4
NY, NX = 4, 4
NCH = 4
HUBS = (8, 5, 11, 2, 14)
UNROLL = 4
HA, HB = 64, 128
FW = 256
FE = 128
MESH = pl.DeviceIdType.MESH
epsilon = 1e-06
theta_base = 10000.0
LOG2E = 1.4426950408889634


def rcopy(src, dst, send_sem, recv_sem, device):
    return pltpu.make_async_remote_copy(
        src_ref=src,
        dst_ref=dst,
        send_sem=send_sem,
        recv_sem=recv_sem,
        device_id=device,
        device_id_type=MESH,
    )


def landed(ref, sem):
    pltpu.make_async_copy(ref, ref, sem).wait()


def dot_t(a, b):
    return lax.dot_general(a, b, (((1,), (1,)), ((), ())), preferred_element_type=jnp.float32)


def dot_n(a, b):
    return jnp.dot(a, b, preferred_element_type=jnp.float32)


def dot_exact(a, b, dims):
    return lax.dot_general(
        a,
        b,
        (dims, ((), ())),
        preferred_element_type=jnp.float32,
        precision=lax.Precision.HIGHEST,
    )


def layer_kernel(
    dims,
    loads,
    lq_ref,
    lk_ref,
    lv_ref,
    lg_ref,
    bq_ref,
    bk_ref,
    bv_ref,
    bg_ref,
    tok_ref,
    wl_ref,
    wb_ref,
    gate_ref,
    up_ref,
    down_ref,
    mg_ref,
    cg_ref,
    re_ref,
    rl_ref,
    gw_ref,
    o_ref,
    q_ref,
    kvl_ref,
    kvb_ref,
    qbuf,
    kvl,
    kvb,
    osl,
    osb,
    obl,
    obb,
    lsend,
    lbuf,
    wo,
    wgu,
    wd,
    msend,
    mbuf,
    stsend,
    stbuf,
    psend,
    pbuf,
    st2send,
    st2buf,
    stream,
    sel0,
    sel1,
    sel_wide,
    scsend,
    scbuf,
    outgo,
    xbuf,
    rsend,
    rbuf,
    gown,
    hbuf,
    dsend,
    dbuf,
    down_own,
    eout,
    ret,
    q_s,
    q_r,
    kv_s,
    kv_r,
    kv_f,
    o_s,
    o_r,
    wo_s,
    wo_r,
    wg_s,
    wg_r,
    wd_s,
    wd_r,
    loc,
    m_s,
    m_r,
    st_s,
    st_r,
    p_s,
    p_r,
    st2_s,
    st2_r,
    d_s,
    d_r,
    sc_s,
    sc_r,
    ya_s,
    ya_r,
    rx_s,
    rx_r,
    hx_s,
    hx_r,
    ry_s,
    ry_r,
    b_s,
    b_r,
):
    nz, ny, nx, t, cap = dims
    nsp = nz * 2
    ntp = ny * nx
    half = ny // KV
    grp = nx
    nb = nsp // grp
    cb = nsp // NCH
    rows = cb * cap
    wide = 32 if cap <= 32 else 128
    per = 128 // wide
    z, c = lax.axis_index("z"), lax.axis_index("c")
    y, x = lax.axis_index("y"), lax.axis_index("x")
    s = z * 2 + c
    tp = y * nx + x
    head = y // half
    j = x
    bf16, f32 = jnp.bfloat16, jnp.float32

    def member(g):
        return (z, c, y, g)

    def tp_dev(n):
        return (z, c, n // nx, n % nx)

    def sp_dev(n):
        return (n // 2, n % 2, y, x)

    barrier = pltpu.get_barrier_semaphore()
    for d in range(1, nsp):
        pl.semaphore_signal(barrier, inc=1, device_id=sp_dev((s + d) % nsp), device_id_type=MESH)
    for d in range(1, ntp):
        pl.semaphore_signal(barrier, inc=1, device_id=tp_dev((tp + d) % ntp), device_id_type=MESH)

    for copy in loads:
        copy.wait()

    def turned(raw, swapped, gain, size):
        quarter = size // 4
        lane = lax.broadcasted_iota(jnp.int32, (t, 128), 1)
        at = lax.broadcasted_iota(jnp.int32, (t, 128), 0) + s * t
        spot = jnp.where(lane < size // 2, at >> GRID_BITS, at & (GRID_W - 1)).astype(f32)
        step = (lane & (quarter - 1)).astype(f32) * (-math.log(theta_base) / quarter)
        angle = spot * jnp.exp(step)
        cosine = jnp.cos(angle)
        sine = jnp.where((lane & quarter) == 0, -1.0, 1.0) * jnp.sin(angle)
        results = []
        for (a, b), (g, h) in zip(zip(raw, swapped), gain):
            scale = lax.rsqrt(jnp.sum(a * a, axis=1, keepdims=True) * (1.0 / size) + epsilon)
            results.append(scale * (a * (g * cosine) + b * (h * sine)))
        return results

    def unit(size, shift):
        row = lax.broadcasted_iota(jnp.int32, (size, 128), 0)
        lane = lax.broadcasted_iota(jnp.int32, (size, 128), 1)
        return row + shift == lane, row == (lane ^ (size // 4))

    def gain_pair(ref, swap):
        pairs = dot_exact(ref[...], swap, ((1,), (0,)))
        return pairs[0:1], pairs[1:2]

    first = ((0,), (0,))

    def flipped(array, matrix):
        return lax.dot_general(array, matrix, (first, ((), ())), preferred_element_type=f32)

    same, swap = unit(HA, 0)
    place, _ = unit(HA, HA)
    same_b, swap_b, place_b = same.astype(bf16), swap.astype(bf16), place.astype(bf16)
    lk = lk_ref[head]
    g_raw, g_swap = gain_pair(lg_ref, same.astype(f32)), gain_pair(lg_ref, swap.astype(f32))
    q_a, k_a = turned(
        (flipped(lq_ref[...], same_b), flipped(lk, same_b)),
        (flipped(lq_ref[...], swap_b), flipped(lk, swap_b)),
        tuple(zip(g_raw, g_swap)),
        HA,
    )
    q_ref[:, 0:128] = q_a.astype(bf16)
    kvl_ref[...] = (k_a + flipped(lv_ref[head], place_b)).astype(bf16)
    _, swap = unit(HB, 0)
    swap_b = swap.astype(bf16)
    pair_row = lax.broadcasted_iota(jnp.int32, (t, KV * t), 0) * KV + head
    pick = (pair_row == lax.broadcasted_iota(jnp.int32, (t, KV * t), 1)).astype(bf16)
    k_raw = dot_n(pick, bk_ref[...])
    g_raw = (bg_ref[0:1], bg_ref[1:2])
    q_b, k_b = turned(
        (bq_ref[...].astype(f32), k_raw),
        (dot_n(bq_ref[...], swap_b), dot_n(k_raw.astype(bf16), swap_b)),
        tuple(zip(g_raw, gain_pair(bg_ref, swap.astype(f32)))),
        HB,
    )
    q_ref[:, 128:256] = q_b.astype(bf16)
    kvb_ref[:, 0:128] = k_b.astype(bf16)
    kvb_ref[:, 128:256] = dot_n(pick, bv_ref[...]).astype(bf16)

    experts = lax.broadcasted_iota(jnp.int32, (nsp, t), 0)
    e0 = (experts == re_ref[0:1]).astype(f32)
    e1 = (experts == re_ref[1:2]).astype(f32)
    before = (
        lax.broadcasted_iota(jnp.int32, (t, t), 0) < lax.broadcasted_iota(jnp.int32, (t, t), 1)
    ).astype(bf16)
    rank = dot_n((e0 + e1).astype(bf16), before)

    def slots(pitch):
        row = lax.broadcasted_iota(jnp.int32, (nsp * pitch, t), 0)
        place = rank + (experts * pitch).astype(f32)
        for e in (e0, e1):
            slot = jnp.sum(e * place, axis=0, keepdims=True).astype(jnp.int32)
            yield (row == slot).astype(f32)

    for part, sel in zip(slots(cap), (sel0, sel1)):
        sel[...] = part.astype(bf16)
    sel_wide[...] = sum(slots(wide)).astype(bf16)
    wo[:, :, 0] = jnp.zeros_like(wo[:, :, 0])
    qbuf[j] = q_ref[...]

    pl.semaphore_wait(barrier, nsp - 1 + ntp - 1)

    def send(src, dst, send_sem, recv_sem, device):
        copy = rcopy(src, dst, send_sem, recv_sem, device)
        copy.start()

    source = s % grp == j
    mine = s // grp
    hubs = HUBS if nz == 16 else tuple(range(1, nz))
    kv_pairs = ((kvl_ref, kvl), (kvb_ref, kvb))

    @pl.when(source)
    def _():
        for part, (src, dst) in enumerate(kv_pairs):
            for n, d in enumerate(hubs):
                rcopy(
                    src,
                    dst.at[mine],
                    kv_s.at[part],
                    kv_r.at[part, mine],
                    ((z + d) % nz, mine % 2, y, x),
                ).start()
            rcopy(
                src, dst.at[mine], kv_s.at[part], kv_r.at[part, mine], (z, 1 - c, y, x)
            ).start()

    for d in range(1, grp):
        g = (j + d) % grp
        send(q_ref, qbuf.at[j], q_s.at[0], q_r.at[0], member(g))

    locals_ = []

    def local(src, dst, n):
        copy = pltpu.make_async_copy(src, dst, loc.at[n])
        copy.start()
        locals_.append(copy)

    local(wl_ref.at[pl.ds(y * nx, nx)], wo.at[y, :, 1], 0)
    local(wb_ref.at[pl.ds(ntp // 2 + y * nx, nx)], wo.at[y, :, pl.ds(2, 2)], 1)
    local(gate_ref.at[:, x], wgu.at[x, :, :, pl.ds(0, FE)], 2)
    for d in range(1, ny):
        to = (y + d) % ny
        dev = (z, c, to, x)
        send(wl_ref.at[pl.ds(to * nx, nx)], wo.at[y, :, 1], wo_s.at[0], wo_r.at[0], dev)
        send(
            wb_ref.at[pl.ds(ntp // 2 + to * nx, nx)],
            wo.at[y, :, pl.ds(2, 2)],
            wo_s.at[1],
            wo_r.at[1],
            dev,
        )
    for d in range(1, nx):
        to = (x + d) % nx
        dev = (z, c, y, to)
        send(gate_ref.at[:, to], wgu.at[x, :, :, pl.ds(0, FE)], wg_s.at[0], wg_r.at[0], dev)

    def send_up(d):
        to = (x + d) % nx
        dev = (z, c, y, to)
        send(up_ref.at[:, to], wgu.at[x, :, :, pl.ds(FE, FE)], wg_s.at[1], wg_r.at[1], dev)

    near_x = sorted({1, nx - 1})
    for d in near_x:
        send_up(d)

    for d in range(1, ny):
        to = (y + d) % ny
        send(down_ref.at[to], wd.at[y], wd_s.at[0], wd_r.at[0], (z, c, to, x))

    local(up_ref.at[:, x], wgu.at[x, :, :, pl.ds(FE, FE)], 3)
    local(down_ref.at[y], wd.at[y], 4)

    def away(i):
        return (z - (i * grp + j) // 2 + nz) % nz

    def hub(i):
        return (c == i % 2) & (away(i) % 3 == 2) if nz == 16 else away(i) < 0

    def pass_on(part, i):
        dst = kv_pairs[part][1]
        landed(dst.at[i], kv_r.at[part, i])

        @pl.when((c == i % 2) & (away(i) != 0))
        def _():
            rcopy(
                dst.at[i], dst.at[i], kv_f.at[part, i], kv_r.at[part, i], (z, 1 - c, y, x)
            ).start()

    def arrive_first(part):
        src, dst = kv_pairs[part]
        for i in range(nb):

            @pl.when((mine == i) & source)
            def _():
                dst[i] = src[...]

            @pl.when(hub(i))
            def _():
                pass_on(part, i)
                for d in (1, nz - 1):
                    rcopy(
                        dst.at[i],
                        dst.at[i],
                        kv_f.at[part, i],
                        kv_r.at[part, i],
                        ((z + d) % nz, c, y, x),
                    ).start()

    def arrive(part):
        for i in range(nb):
            direct = ((mine == i) & source) | hub(i)

            @pl.when(jnp.logical_not(direct))
            def _():
                pass_on(part, i)

    arrive_first(0)
    arrive_first(1)
    arrive(0)
    landed(qbuf.at[pl.ds(0, grp - 1)], q_r.at[0])

    scale_a = HA**-0.5 * LOG2E
    scale_b = HB**-0.5 * LOG2E
    lane_a = lax.broadcasted_iota(jnp.int32, (t, 128), 1)

    def attend(scores, values, scale):
        peak = jnp.max(scores, axis=1, keepdims=True) * scale
        weights = jnp.exp2(scores * scale - peak)
        total = jnp.sum(weights, axis=1, keepdims=True)
        out = dot_n(weights.astype(bf16), values) / total
        return out, peak + jnp.log(total) * LOG2E

    def split3(v):
        a = v.astype(bf16).astype(f32)
        b = (v - a).astype(bf16).astype(f32)
        return a, b, v - a - b

    def marked(value, lse, at):
        for n, piece in enumerate(split3(lse)):
            value = jnp.where(lane_a == at + n, piece, value)
        return value

    def hand_over(part, src, dst, d, g):
        @pl.when(d < grp)
        def _():
            rcopy(src.at[g], dst.at[j], o_s.at[part], o_r.at[part], member(g)).start()

        @pl.when(d == grp)
        def _():
            dst[j] = src[g]

    def lean_head(d, carry):
        g = (j + d) % grp
        kv_l = kvl[...].reshape(nb * t, 128)
        out, lse = attend(dot_t(qbuf[g, :, 0:128], kv_l), kv_l, scale_a)
        osl[g] = marked(out, lse, 0).astype(bf16)
        hand_over(0, osl, obl, d, g)
        return carry

    def broad_head(d, lses):
        g = (j + d) % grp
        k_b = kvb[:, :, 0:128].reshape(nb * t, 128)
        v_b = kvb[:, :, 128:256].reshape(nb * t, 128)
        out, lse = attend(dot_t(qbuf[g, :, 128:256], k_b), v_b, scale_b)
        osb[g] = out.astype(bf16)
        hand_over(1, osb, obb, d, g)
        return jnp.where(lane_a == g, lse, lses)

    lax.fori_loop(1, grp + 1, lean_head, 0, unroll=UNROLL)
    arrive(1)
    lses = lax.fori_loop(1, grp + 1, broad_head, jnp.zeros((t, 128), f32), unroll=UNROLL)
    last = ((1,), (1,))
    row8 = lax.broadcasted_iota(jnp.int32, (8, 128), 0)
    eye8 = (row8 == lax.broadcasted_iota(jnp.int32, (8, 128), 1)).astype(f32)
    lsend[...] = jnp.zeros_like(lsend)
    lse_rows = dot_exact(eye8, lses, last)
    for g in range(grp):
        lsend[g, :, 0:t] = lse_rows[g : g + 1]
    for d in range(1, grp):
        g = (j + d) % grp
        send(lsend.at[g], lbuf.at[j], o_s.at[2], o_r.at[2], member(g))
    lbuf[j] = lsend[j]

    landed(obl.at[pl.ds(0, grp - 1)], o_r.at[0])
    landed(obb.at[pl.ds(0, grp - 1)], o_r.at[1])
    landed(lbuf.at[pl.ds(0, grp - 1)], o_r.at[2])

    row_g = lax.broadcasted_iota(jnp.int32, (8, t), 0)
    lse_rows = jnp.zeros((8, t), f32)
    for g in range(grp):
        lse_rows = jnp.where(row_g == g, lbuf[g, :, 0:t], lse_rows)
    lse_cols = dot_exact(lse_rows, eye8, first)
    lses = []
    for g in range(grp):
        stats = obl[g].astype(f32)
        lses.append(
            (stats[:, 0:1] + stats[:, 1:2] + stats[:, 2:3], lse_cols[:, g : g + 1])
        )
    top_a = functools.reduce(jnp.maximum, [v[0] for v in lses])
    top_b = functools.reduce(jnp.maximum, [v[1] for v in lses])
    sum_a, sum_b = 0.0, 0.0
    acc_a, acc_b = 0.0, 0.0
    for g in range(grp):
        wa = jnp.exp2(lses[g][0] - top_a)
        wb = jnp.exp2(lses[g][1] - top_b)
        sum_a, sum_b = sum_a + wa, sum_b + wb
        acc_a = acc_a + wa * obl[g].astype(f32)
        acc_b = acc_b + wb * obb[g].astype(f32)
    head_a = jnp.where(lane_a >= HA, acc_a / sum_a, 0.0).astype(bf16)
    head_b = (acc_b / sum_b).astype(bf16)
    msend[:, 0:128] = head_a
    msend[:, 128:256] = head_b
    pick_a = (row8 == 0).astype(f32)
    pick_b = (row8 == 1).astype(f32)
    sq_a, sq_b = head_a.astype(f32), head_b.astype(f32)
    stsend[...] = jnp.zeros_like(stsend)
    squares = dot_exact(pick_a, sq_a * sq_a, last) + dot_exact(pick_b, sq_b * sq_b, last)
    stsend[:, 0:t] = squares[0:2]
    for d in range(1, ntp):
        n = (tp + d) % ntp
        send(stsend, stbuf.at[tp], st_s.at[0], st_r.at[0], tp_dev(n))
    stbuf[tp] = stsend[...]
    for d in range(1, nx):
        to = (x + d) % nx
        send(msend, mbuf.at[x], m_s.at[0], m_r.at[0], (z, c, y, to))
    mbuf[x] = msend[...]
    landed(stbuf.at[pl.ds(0, ntp - 1)], st_r.at[0])
    sums = jnp.sum(stbuf[...], axis=0)[:, 0:t]
    row_t = lax.broadcasted_iota(jnp.int32, (8, t), 0)
    sums = jnp.where(row_t == 0, sums[0:1] * (1.0 / (ntp * HA)), sums[1:2] * (1.0 / (ntp * HB)))
    inverse = lax.rsqrt(sums + epsilon)
    norm_a = dot_exact(inverse, pick_a, first)
    norm_b = dot_exact(inverse, pick_b, first)
    landed(mbuf.at[pl.ds(0, nx - 1)], m_r.at[0])
    for copy in locals_:
        copy.wait()
    landed(wo.at[pl.ds(0, ny - 1), :, 1], wo_r.at[0])
    landed(wo.at[pl.ds(0, ny - 1), :, pl.ds(2, 2)], wo_r.at[1])
    for n in range(nx):
        gain = mg_ref[pl.ds((y * nx + n) // 2, 1)]
        if n % 2 == 0:
            gain = pltpu.roll(gain, HA, 1)
        part = mbuf[n]
        mbuf[n, :, 0:128] = (part[:, 0:128].astype(f32) * norm_a * gain).astype(bf16)
        gain = mg_ref[pl.ds(ntp // 2 + y * nx + n, 1)]
        mbuf[n, :, 128:256] = (part[:, 128:256].astype(f32) * norm_b * gain).astype(bf16)

    def project(n):
        acc = dot_n(mbuf[0], wo[n, 0].reshape(FW, FW))
        for m in range(1, nx):
            acc = acc + dot_n(mbuf[m], wo[n, m].reshape(FW, FW))
        return acc

    for d in range(1, ny):
        to = (y + d) % ny
        psend[d] = project(to).astype(bf16)
        send(psend.at[d], pbuf.at[y], p_s.at[0], p_r.at[0], (z, c, to, x))
    for d in range(1, nx):
        if d not in near_x:
            send_up(d)
    total = tok_ref[...].astype(f32) + project(y)
    landed(pbuf.at[pl.ds(0, ny - 1)], p_r.at[0])
    for d in range(1, ny):
        n = (y + d) % ny
        total = total + pbuf[n].astype(f32)
    stream[...] = total
    ones8 = jnp.ones((8, FW), f32)
    st2send[...] = jnp.zeros_like(st2send)
    st2send[:, 0:t] = dot_exact(ones8, total * total, last)[0:1]
    for d in range(1, ntp):
        n = (tp + d) % ntp
        send(st2send, st2buf.at[tp], st2_s.at[0], st2_r.at[0], tp_dev(n))
    st2buf[tp] = st2send[...]

    feats = (total * cg_ref[...]).astype(bf16)
    picked = dot_n(sel0[...] + sel1[...], feats).astype(bf16)
    for n in range(nsp):
        outgo[n] = picked[n * cap : (n + 1) * cap]
    near = s // cb

    def dispatch(n, part):
        send(outgo.at[n], xbuf.at[y, s], d_s.at[part], d_r.at[near], sp_dev(n))

    def dispatch_far(far):
        for i in range(cb):
            for d in sorted({NCH - far, far}, reverse=True):
                dispatch((near + d) % NCH * cb + i, 1)

    for d in range(1, cb):
        dispatch(near * cb + (s + d) % cb, 0)
    landed(outgo.at[pl.ds(0, cb - 1)], d_s.at[0])
    xbuf[y, s] = outgo[s]
    for far in range(1, NCH // 2):
        dispatch_far(far)
    landed(st2buf.at[pl.ds(0, ntp - 1)], st2_r.at[0])
    squares = jnp.sum(st2buf[...], axis=0)[:, 0:t]
    inverse = lax.rsqrt(squares * (1.0 / (ntp * FW)) + epsilon)
    inverse = jnp.broadcast_to(inverse, (8, t))
    parts = split3(inverse)
    split = jnp.where(row_t == 0, parts[0], jnp.where(row_t == 1, parts[1], parts[2]))
    split = jnp.where(row_t < 3, split, 0.0).astype(bf16)
    factors = jnp.sum(dot_t(split, sel_wide[...]), axis=0, keepdims=True)
    for n in range(nsp // per):
        scsend[n] = factors[:, n * 128 : (n + 1) * 128]
    for d in range(1, nsp):
        n = (s + d) % nsp
        send(scsend.at[n // per], scbuf.at[s], sc_s.at[0], sc_r.at[near], sp_dev(n))
    scbuf[s] = scsend[s // per]
    dispatch_far(NCH // 2)

    def chunk(k):
        return (near + NCH + (k + 1) // 2 * (2 * (k % 2) - 1)) % NCH

    def stage_a(k):
        ch = chunk(k)
        landed(xbuf.at[y, pl.ds(0, cb - (k == 0))], d_r.at[ch])
        part = xbuf.at[y, pl.ds(ch * cb, cb)]
        for d in range(1, ny):
            to = (y + d) % ny
            rcopy(part, part, ya_s.at[0], ya_r.at[ch], (z, c, to, x)).start()

    def stage_b(k):
        ch = chunk(k)
        landed(xbuf.at[pl.ds(0, ny - 1), pl.ds(0, cb)], ya_r.at[ch])

        @pl.when(k == 0)
        def _():
            for n in range(2):
                landed(wgu.at[pl.ds(0, nx - 1), :, :, pl.ds(n * FE, FE)], wg_r.at[n])

        xs = [xbuf[n, pl.ds(ch * cb, cb)].reshape(rows, FW) for n in range(ny)]

        def expand(n):
            acc = dot_n(xs[0], wgu[n, 0])
            for m in range(1, ny):
                acc = acc + dot_n(xs[m], wgu[n, m])
            return acc

        for d in range(1, nx):
            to = (x + d) % nx
            rsend[ch, d] = expand(to).astype(bf16)
            rcopy(
                rsend.at[ch, d], rbuf.at[ch, x], rx_s.at[0], rx_r.at[ch], (z, c, y, to)
            ).start()
        gown[ch] = expand(x)

    def stage_c(k):
        ch = chunk(k)
        both = gown[ch]
        landed(rbuf.at[ch, pl.ds(0, nx - 1)], rx_r.at[ch])
        for d in range(1, nx):
            n = (x + d) % nx
            both = both + rbuf[ch, n].astype(f32)
        row = lax.broadcasted_iota(jnp.int32, (cap, 128), 0)
        spot = row + s % per * wide == lax.broadcasted_iota(jnp.int32, (cap, 128), 1)
        factor = []

        @pl.when(k == 0)
        def _():
            landed(scbuf.at[pl.ds(0, cb - 1)], sc_r.at[ch])

        @pl.when(k > 0)
        def _():
            landed(scbuf.at[pl.ds(0, cb)], sc_r.at[ch])

        for i in range(cb):
            b = ch * cb + i
            value = jnp.where(spot, scbuf[b], 0.0)
            factor.append(jnp.sum(value, axis=1, keepdims=True))
        both = both * jnp.concatenate(factor, axis=0)
        gate_value = both[:, 0:FE]
        hidden = (gate_value / (1.0 + jnp.exp(-gate_value)) * both[:, FE:]).astype(bf16)
        hbuf[ch, x] = hidden
        for d in range(1, nx):
            to = (x + d) % nx
            rcopy(
                hbuf.at[ch, x], hbuf.at[ch, x], hx_s.at[0], hx_r.at[ch], (z, c, y, to)
            ).start()

    def stage_d(k):
        ch = chunk(k)
        landed(hbuf.at[ch, pl.ds(0, nx - 1)], hx_r.at[ch])

        @pl.when(k == 0)
        def _():
            landed(wd.at[pl.ds(0, ny - 1)], wd_r.at[0])

        wide = jnp.concatenate([hbuf[ch, n] for n in range(nx)], axis=1)
        for d in range(1, ny):
            to = (y + d) % ny
            dsend[ch, d] = dot_n(wide, wd[to]).astype(bf16)
            rcopy(
                dsend.at[ch, d], dbuf.at[ch, y], ry_s.at[0], ry_r.at[ch], (z, c, to, x)
            ).start()
        down_own[ch] = dot_n(wide, wd[y])

    def stage_e(k):
        ch = chunk(k)
        acc = down_own[ch]
        landed(dbuf.at[ch, pl.ds(0, ny - 1)], ry_r.at[ch])
        for d in range(1, ny):
            n = (y + d) % ny
            acc = acc + dbuf[ch, n].astype(f32)
        eout[pl.ds(ch * cb, cb)] = acc.astype(bf16).reshape(cb, cap, FW)
        for i in range(cb):
            b = ch * cb + i

            @pl.when(b != s)
            def _():
                rcopy(eout.at[b], ret.at[s], b_s.at[0], b_r.at[0], sp_dev(b)).start()

            @pl.when(b == s)
            def _():
                ret[s] = eout[b]


    stages = (stage_a, stage_b, stage_c, stage_d, stage_e)

    behind = ((0, 0), (1, 1), (1, 2), (2, 3)) if NCH == 4 else tuple((k, k) for k in range(NCH))

    def step(i, carry):
        for lag in (4, 3, 2, 1):

            @pl.when((i >= lag) & (i < NCH + lag))
            def _():
                stages[lag](i - lag)

        for at, k in behind:

            @pl.when(i == at)
            def _():
                stage_a(k)

        return carry

    lax.fori_loop(0, NCH + len(stages) - 1, step, 0)

    landed(ret.at[pl.ds(0, nsp - 1)], b_r.at[0])
    back = ret[...].reshape(nsp * cap, FW)
    gap = rl_ref[0:1] - rl_ref[1:2]
    w0 = gw_ref[...] / (1.0 + jnp.exp(-gap))
    w1 = gw_ref[...] / (1.0 + jnp.exp(gap))
    both = jnp.where(row_t == 0, w0, jnp.where(row_t == 1, w1, 0.0))
    w0, w1 = dot_exact(both, pick_a, first), dot_exact(both, pick_b, first)
    w0, w1 = jnp.concatenate([w0, w0], axis=1), jnp.concatenate([w1, w1], axis=1)
    routed = w0 * flipped(sel0[...], back) + w1 * flipped(sel1[...], back)
    o_ref[...] = stream[...] + routed


    for part, (src, dst) in enumerate(kv_pairs):

        @pl.when(source)
        def _():
            landed(dst.at[pl.ds(0, len(hubs) + 1)], kv_s.at[part])

        for i in range(nb):

            @pl.when(hub(i))
            def _():
                landed(dst.at[pl.ds(0, min(3, nb))], kv_f.at[part, i])

            @pl.when((c == i % 2) & (away(i) != 0) & jnp.logical_not(hub(i)))
            def _():
                landed(dst.at[i], kv_f.at[part, i])

    landed(qbuf.at[pl.ds(0, grp - 1)], q_s.at[0])
    for n in range(2):
        landed(((obl, obb)[n]).at[pl.ds(0, grp - 1)], o_s.at[n])
    landed(lbuf.at[pl.ds(0, grp - 1)], o_s.at[2])
    landed(wo.at[pl.ds(0, ny - 1), :, 1], wo_s.at[0])
    landed(wo.at[pl.ds(0, ny - 1), :, pl.ds(2, 2)], wo_s.at[1])
    for n in range(2):
        landed(wgu.at[pl.ds(0, nx - 1), :, :, pl.ds(n * FE, FE)], wg_s.at[n])
    landed(wd.at[pl.ds(0, ny - 1)], wd_s.at[0])
    landed(mbuf.at[pl.ds(0, nx - 1)], m_s.at[0])
    landed(stbuf.at[pl.ds(0, ntp - 1)], st_s.at[0])
    landed(pbuf.at[pl.ds(0, ny - 1)], p_s.at[0])
    landed(st2buf.at[pl.ds(0, ntp - 1)], st2_s.at[0])
    landed(outgo.at[pl.ds(0, nsp - cb)], d_s.at[1])
    landed(scbuf.at[pl.ds(0, nsp - 1)], sc_s.at[0])
    landed(xbuf.at[pl.ds(0, ny - 1)], ya_s.at[0])
    landed(rbuf.at[:, pl.ds(0, nx - 1)], rx_s.at[0])
    landed(hbuf.at[:, pl.ds(0, nx - 1)], hx_s.at[0])
    landed(dbuf.at[:, pl.ds(0, ny - 1)], ry_s.at[0])
    landed(ret.at[pl.ds(0, nsp - 1)], b_s.at[0])


SMALL = (*range(9), *range(14, 19))


def entry(dims, *refs):
    inputs, rest = list(refs[:19]), refs[19 : -len(SMALL) - 1]
    loads = []
    for n, (i, held) in enumerate(zip(SMALL, refs[-len(SMALL) - 1 : -1])):
        copy = pltpu.make_async_copy(inputs[i], held, refs[-1].at[n])
        copy.start()
        loads.append(copy)
        inputs[i] = held
    layer_kernel(dims, loads, *inputs, *rest)


def on_device(
    tokens,
    lean_query,
    lean_key,
    lean_value,
    lean_gains,
    broad_query,
    broad_key,
    broad_value,
    broad_gains,
    mixer_gain,
    output_weight,
    channel_gain,
    gate_weight,
    up_weight,
    down_weight,
    route_experts,
    route_logits,
    group_weight,
):
    nz, ny, nx = lax.axis_size("z"), lax.axis_size("y"), lax.axis_size("x")
    nsp, ntp = nz * 2, ny * nx
    t = tokens.shape[0]
    cap = t // (nsp // GROUPS)
    wide = 32 if cap <= 32 else 128
    half = ny // KV
    grp = nx
    nb = nsp // grp
    cb = nsp // NCH
    rows = cb * cap
    bf16, f32 = jnp.bfloat16, jnp.float32
    vm = pl.BlockSpec(memory_space=pltpu.VMEM)
    hbm = pl.BlockSpec(memory_space=pl.ANY)
    dma = pltpu.SemaphoreType.DMA
    inputs = (
        lean_query.transpose(1, 2, 0)[0],
        lean_key.transpose(1, 2, 0),
        lean_value.transpose(1, 2, 0),
        lean_gains,
        broad_query[:, 0],
        broad_key.reshape(KV * t, HB),
        broad_value.reshape(KV * t, HB),
        broad_gains,
        tokens,
        output_weight.reshape(3 * ntp, 64, FW),
        output_weight.reshape(3 * ntp // 2, 2, 64, FW),
        gate_weight.reshape(ny, nx, FW, FE),
        up_weight.reshape(ny, nx, FW, FE),
        down_weight.reshape(ny, nx * FE, FW),
        mixer_gain.reshape(-1, 128),
        channel_gain.reshape(1, FW),
        route_experts.T,
        route_logits.T,
        group_weight.reshape(1, t),
    )
    return pl.pallas_call(
        functools.partial(entry, (nz, ny, nx, t, cap)),
        out_shape=jax.ShapeDtypeStruct((t, FW), f32),
        in_specs=[hbm] * 19,
        out_specs=vm,
        scratch_shapes=[
            pltpu.VMEM((t, 256), bf16),
            pltpu.VMEM((t, 128), bf16),
            pltpu.VMEM((t, 256), bf16),
            pltpu.VMEM((grp, t, 256), bf16),
            pltpu.VMEM((nb, t, 128), bf16),
            pltpu.VMEM((nb, t, 256), bf16),
            pltpu.VMEM((grp, t, 128), bf16),
            pltpu.VMEM((grp, t, 128), bf16),
            pltpu.VMEM((grp, t, 128), bf16),
            pltpu.VMEM((grp, t, 128), bf16),
            pltpu.VMEM((8, 1, 256), f32),
            pltpu.VMEM((grp, 1, 256), f32),
            pltpu.VMEM((ny, nx, 4, 64, FW), bf16),
            pltpu.VMEM((nx, ny, FW, FW), bf16),
            pltpu.VMEM((ny, nx * FE, FW), bf16),
            pltpu.VMEM((t, 256), bf16),
            pltpu.VMEM((nx, t, 256), bf16),
            pltpu.VMEM((2, 256), f32),
            pltpu.VMEM((ntp, 2, 256), f32),
            pltpu.VMEM((ny, t, FW), bf16),
            pltpu.VMEM((ny, t, FW), bf16),
            pltpu.VMEM((1, 256), f32),
            pltpu.VMEM((ntp, 1, 256), f32),
            pltpu.VMEM((t, FW), f32),
            pltpu.VMEM((nsp * cap, t), bf16),
            pltpu.VMEM((nsp * cap, t), bf16),
            pltpu.VMEM((nsp * wide, t), bf16),
            pltpu.VMEM((nsp * wide // 128, 1, 128), f32),
            pltpu.VMEM((nsp, 1, 128), f32),
            pltpu.VMEM((nsp, cap, FW), bf16),
            pltpu.VMEM((ny, nsp, cap, FW), bf16),
            pltpu.VMEM((NCH, nx, rows, FW), bf16),
            pltpu.VMEM((NCH, nx, rows, FW), bf16),
            pltpu.VMEM((NCH, rows, FW), f32),
            pltpu.VMEM((NCH, nx, rows, FE), bf16),
            pltpu.VMEM((NCH, ny, rows, FW), bf16),
            pltpu.VMEM((NCH, ny, rows, FW), bf16),
            pltpu.VMEM((NCH, rows, FW), f32),
            pltpu.VMEM((nsp, cap, FW), bf16),
            pltpu.VMEM((nsp, cap, FW), bf16),
            dma((1,)),
            dma((1,)),
            dma((2,)),
            dma((2, nb)),
            dma((2, nb)),
            dma((3,)),
            dma((3,)),
            dma((2,)),
            dma((2,)),
            dma((2,)),
            dma((2,)),
            dma((1,)),
            dma((1,)),
            dma((5,)),
            dma((1,)),
            dma((1,)),
            dma((1,)),
            dma((1,)),
            dma((1,)),
            dma((1,)),
            dma((1,)),
            dma((1,)),
            dma((2,)),
            dma((NCH,)),
            dma((1,)),
            dma((NCH,)),
            dma((1,)),
            dma((NCH,)),
            dma((1,)),
            dma((NCH,)),
            dma((1,)),
            dma((NCH,)),
            dma((1,)),
            dma((NCH,)),
            dma((1,)),
            dma((1,)),
            *(pltpu.VMEM(inputs[i].shape, inputs[i].dtype) for i in SMALL),
            dma((len(SMALL),)),
        ],
        compiler_params=pltpu.CompilerParams(
            collective_id=0, has_side_effects=True, vmem_limit_bytes=60 * 1024 * 1024
        ),
    )(*inputs).astype(bf16)


def solution(mesh):
    finer = Mesh(
        mesh.devices.reshape(mesh.shape["sp"] // 2, 2, NY, NX), ("z", "c", "y", "x")
    )
    sp, tp = ("z", "c"), ("y", "x")
    return jax.shard_map(
        on_device,
        mesh=finer,
        in_specs=(
            P(sp, tp),
            P(sp, tp, None),
            P(sp, None, None),
            P(sp, None, None),
            P(),
            P(sp, tp, None),
            P(sp, None, None),
            P(sp, None, None),
            P(),
            P(),
            P(None, tp),
            P(tp),
            P(sp, None, tp),
            P(sp, None, tp),
            P(sp, None, tp),
            P(sp, None),
            P(sp, None),
            P(sp),
        ),
        out_specs=P(sp, tp),
        check_vma=False,
    )
```
